512 devices in a mesh: sp: 16 (over z), tp: 4 (over y), dp: 8 (over x, core).
Axes of the slice: x: 4, y: 4, z: 16, core: 2. Of those that a mesh axis runs over, the one named last changes fastest.
Arguments:
- latent: bfloat16 [32768, 2048], P(('dp', 'sp', 'tp')), parts along dimension 0, may hold values from -6 to 6
- context: bfloat16 [2048, 2048], P(('dp', 'sp')), parts along dimension 0, may hold values from -6 to 6
- cond: bfloat16 [16384], P(('dp', 'sp')), parts along dimension 0, may hold values from -6 to 6
- context_cond: bfloat16 [2048], P('sp'), may hold values from -6 to 6
- norm_gain: float32 [2048], replicated, may hold values from 0.1 to 1.9
- mod_shift: bfloat16 [2048, 2048], P('sp', 'tp'), may hold values from -0.125 to 0.125
- mod_scale: bfloat16 [2048, 2048], P('sp', 'tp'), may hold values from -0.125 to 0.125
- mod_gate: bfloat16 [2048, 2048], P('sp', 'tp'), may hold values from -0.125 to 0.125
- w_query: bfloat16 [2048, 1024], P(None, 'tp'), may hold values from -0.125 to 0.125
- w_key: bfloat16 [2048, 1024], P(None, 'tp'), may hold values from -0.125 to 0.125
- w_value: bfloat16 [2048, 1024], P(None, 'tp'), may hold values from -0.125 to 0.125
- query_gain: float32 [64], replicated, may hold values from 1.4 to 2.2
- key_gain: float32 [64], replicated, may hold values from 0.1 to 1.9
- mix_lambda: float32 [8], P('tp'), may hold values from 0.3 to 0.8
- context_lift: float32 [8], P('tp'), may hold values from 1.5 to 2.5
- value_gain: float32 [128], replicated, may hold values from 0.1 to 1.9
- w_out: bfloat16 [1024, 2048], P('tp'), may hold values from -0.1875 to 0.1875
Outputs:
- output: bfloat16 [32768, 2048], P(('dp', 'sp', 'tp')), parts along dimension 0
The draws below stay inside these ranges and needn't reach their ends.
There are 8 independent parts, one for each index of `dp`. The reference program is written for one: setup_inputs(seed, part) draws one part's arguments, and reference() takes and returns one part's arrays. A program takes and returns all parts, laid end to end along the dimension named above; an argument that names none is the same for every part. Nothing has to cross between parts.
All inputs are finite; a program needn't handle non-finite values.
Results may differ from the reference program's by a relative error of at most 0.006.
Values may be sent and summed in bfloat16 or wider, within the bound.
A program may use at most 64 MiB of HBM per device.

```python
import jax
import jax.numpy as jnp
from jax import lax

D = 2048
HEADS = 8
HEAD_DIM = 64
VALUE_DIM = 128
GRID = 64
CTX = 256
LENGTH = 4096


def levels(key, shape, split, low, largest):
    loudness, own = 1.0, jax.random.fold_in(key, 6)
    for dim, parts in split:
        steps = jnp.exp(jax.random.uniform(jax.random.fold_in(own, dim), (parts,), jnp.float32, low / len(split), largest / len(split)))
        loudness = loudness * jnp.repeat(steps, shape[dim] // parts).reshape([-1 if axis == dim else 1 for axis in range(len(shape))])
    return loudness


def noise(stream_key, extent, width, limit, cuts=(), kind=jnp.bfloat16):
    array = jax.random.normal(stream_key, extent, jnp.float32) * width
    if len(cuts) > 0:
        array = levels(stream_key, extent, cuts, -0.22, 0.18) * array
    return jnp.clip(array, min=-limit, max=limit).astype(kind)


def setup_inputs(seed: int = 0, part: int = 0) -> dict:
    seeds = jax.random.split(jax.random.key(seed), 18)
    part_keys = jax.random.split(jax.random.fold_in(seeds[17], part), 18)
    return {
        "latent": noise(part_keys[0], (LENGTH, D), 1.0, 6.0, ((0, 64),)),
        "context": noise(part_keys[1], (CTX, D), 1.0, 6.0, ((0, 16),)),
        "cond": noise(part_keys[2], (D,), 1.0, 6.0, ((0, 16),)),
        "context_cond": noise(seeds[3], (D,), 1.0, 6.0, ((0, 16),)),
        "norm_gain": jnp.clip(1.0 + 0.18 * jax.random.normal(seeds[4], (D,), jnp.float32), 0.1, 1.9),
        "mod_shift": noise(seeds[5], (D, D), D ** -0.5, 0.125, ((0, 16), (1, 4))),
        "mod_scale": noise(seeds[6], (D, D), D ** -0.5, 0.125, ((0, 16), (1, 4))),
        "mod_gate": noise(seeds[7], (D, D), D ** -0.5, 0.125, ((0, 16), (1, 4))),
        "w_query": noise(seeds[8], (D, 2 * HEADS * HEAD_DIM), D ** -0.5, 0.125, ((1, 4),)),
        "w_key": noise(seeds[9], (D, 2 * HEADS * HEAD_DIM), D ** -0.5, 0.125, ((1, 4),)),
        "w_value": noise(seeds[10], (D, HEADS * VALUE_DIM), D ** -0.5, 0.125, ((1, 4),)),
        "query_gain": jnp.clip(jax.random.uniform(seeds[11], (HEAD_DIM,), jnp.float32, 1.4, 2.2), 1.4, 2.2),
        "key_gain": jnp.clip(1.0 + 0.18 * jax.random.normal(seeds[12], (HEAD_DIM,), jnp.float32), 0.1, 1.9),
        "mix_lambda": jnp.clip(0.3 + 0.5 * jax.random.uniform(seeds[13], (HEADS,), jnp.float32) ** levels(seeds[13], (HEADS,), ((0, 4),), -0.2, 0.2), 0.3, 0.8),
        "context_lift": jnp.clip(1.5 + 1.0 * jax.random.uniform(seeds[14], (HEADS,), jnp.float32) ** levels(seeds[14], (HEADS,), ((0, 4),), -0.2, 0.2), 1.5, 2.5),
        "value_gain": jnp.clip(1.0 + 0.18 * jax.random.normal(seeds[15], (VALUE_DIM,), jnp.float32), 0.1, 1.9),
        "w_out": noise(seeds[16], (HEADS * VALUE_DIM, D), (HEADS * VALUE_DIM) ** -0.5, 0.1875, ((0, 4),)),
    }


token_eps = 0.01
head_eps = 0.001
rope_base = 10000.0
head_factor = 0.8

def modulated_norm(row_block, gain_vector, shift_vector, scale_vector):
    values = row_block.astype(jnp.float32)
    inverse = lax.rsqrt(lax.optimization_barrier(jnp.mean(values * values, axis=-1, keepdims=True)) + token_eps)
    return (values * inverse * gain_vector * (1.0 + scale_vector) + shift_vector).astype(jnp.bfloat16)

def head_norm(values, gain_vector):
    inverse = lax.rsqrt(lax.optimization_barrier(jnp.mean(values * values, axis=-1, keepdims=True)) + token_eps)
    return values * inverse * gain_vector

def rotate(values, positions):
    quarter = values.shape[-1] // 4
    inverse = rope_base ** (-jnp.arange(quarter, dtype=jnp.float32) / quarter)
    grid_row = (positions // GRID).astype(jnp.float32)
    grid_col = (positions % GRID).astype(jnp.float32)
    angles = jnp.stack([grid_row[:, None] * inverse, grid_col[:, None] * inverse], axis=1)
    cosine_table = jnp.cos(angles)[:, None, None]
    sine_table = jnp.sin(angles)[:, None, None]
    halves = values.reshape(values.shape[:3] + (2, 2, quarter))
    front_half = halves[..., 0, :]
    back_half = halves[..., 1, :]
    turned = jnp.stack([front_half * cosine_table - back_half * sine_table, back_half * cosine_table + front_half * sine_table], axis=-2)
    return turned.reshape(values.shape)

def project_heads(row_block, weight, gain_vector, positions, factor):
    row_count = row_block.shape[0]
    head_width = gain_vector.shape[0]
    product = jnp.dot(row_block, weight, preferred_element_type=jnp.float32)
    shaped = head_norm(product.reshape(row_count, -1, 2, head_width), gain_vector)
    if positions is not None:
        shaped = rotate(shaped, positions)
    return (shaped * factor).astype(jnp.bfloat16).reshape(row_count, -1)

def attend_block(query_block, latent_keys, latent_values, context_keys, context_values, mix_lambda, context_lift, value_gain):
    head_count = mix_lambda.shape[0]
    head_width = latent_keys.shape[1] // (2 * head_count)
    shaped_query = query_block.astype(jnp.float32).reshape(query_block.shape[0], head_count, 2, head_width)

    def one_side(key_slab, value_slab, extra):
        shaped_keys = key_slab.astype(jnp.float32).reshape(key_slab.shape[0], head_count, 2, head_width)
        shaped_values = value_slab.astype(jnp.float32).reshape(value_slab.shape[0], head_count, -1)
        scores = jnp.einsum('qhmd,phmd->mhqp', shaped_query, shaped_keys) + extra
        weights = jnp.exp(scores)
        rounded = lax.optimization_barrier(weights.astype(jnp.bfloat16)).astype(jnp.float32)
        return (jnp.einsum('mhqp,phe->mhqe', rounded, shaped_values), lax.optimization_barrier(jnp.sum(weights, axis=-1)))
    latent_numer, latent_total = one_side(latent_keys, latent_values, jnp.float32(0.0))
    context_numer, context_total = one_side(context_keys, context_values, context_lift[None, :, None, None])
    ratios = (latent_numer + context_numer) / (latent_total + context_total)[..., None]
    mixed_heads = ratios[0] - mix_lambda[:, None, None] * ratios[1]
    inverse = lax.rsqrt(lax.optimization_barrier(jnp.mean(mixed_heads * mixed_heads, axis=-1, keepdims=True)) + head_eps)
    normalized = (mixed_heads * inverse * value_gain * head_factor).astype(jnp.bfloat16)
    return jnp.transpose(normalized, (1, 0, 2)).reshape(query_block.shape[0], -1)

def reference(latent, context, cond, context_cond, norm_gain, mod_shift, mod_scale, mod_gate, w_query, w_key, w_value, query_gain, key_gain, mix_lambda, context_lift, value_gain, w_out):
    cond_act = jax.nn.silu(cond.astype(jnp.float32)).astype(jnp.bfloat16)
    context_act = jax.nn.silu(context_cond.astype(jnp.float32)).astype(jnp.bfloat16)
    shift = jnp.dot(cond_act, mod_shift, preferred_element_type=jnp.float32)
    scale = jnp.dot(cond_act, mod_scale, preferred_element_type=jnp.float32)
    gate = jnp.dot(cond_act, mod_gate, preferred_element_type=jnp.float32)
    context_shift = jnp.dot(context_act, mod_shift, preferred_element_type=jnp.float32)
    context_scale = jnp.dot(context_act, mod_scale, preferred_element_type=jnp.float32)
    normed = modulated_norm(latent, norm_gain, shift, scale)
    context_normed = modulated_norm(context, norm_gain, context_shift, context_scale)
    length = latent.shape[0]
    positions = jnp.arange(length, dtype=jnp.int32)
    queries = project_heads(normed, w_query, query_gain, positions, HEAD_DIM ** (-0.5))
    latent_keys = project_heads(normed, w_key, key_gain, positions, 1.0)
    latent_values = jnp.dot(normed, w_value, preferred_element_type=jnp.float32).astype(jnp.bfloat16)
    context_keys = project_heads(context_normed, w_key, key_gain, None, 1.0)
    context_values = jnp.dot(context_normed, w_value, preferred_element_type=jnp.float32).astype(jnp.bfloat16)
    block_rows = 512 if length % 512 == 0 else length
    query_blocks = queries.reshape(length // block_rows, block_rows, -1)
    head_out = lax.map(lambda block_query: attend_block(block_query, latent_keys, latent_values, context_keys, context_values, mix_lambda, context_lift, value_gain), query_blocks).reshape(length, -1)
    mixture = jnp.dot(head_out, w_out, preferred_element_type=jnp.float32)
    return (latent.astype(jnp.float32) + gate * mixture).astype(jnp.bfloat16)
```

```python
import functools

import jax
import jax.numpy as jnp
import numpy as np
from jax import lax
from jax.experimental import pallas as pl
from jax.experimental.pallas import tpu as pltpu
from jax.sharding import PartitionSpec as P

GRID = 64
token_eps = 0.01
head_eps = 0.001
rope_base = 10000.0
head_factor = 0.8
MESH = pl.DeviceIdType.MESH
F32 = jnp.float32
BF16 = jnp.bfloat16


def rope_table(head_width):
    quarter = head_width // 4
    inverse = np.float32(rope_base) ** (-np.arange(quarter, dtype=np.float32) / np.float32(quarter))
    angles = (np.arange(GRID, dtype=np.float32)[:, None] * inverse).astype(np.float64)
    cos, sin = np.cos(angles), np.sin(angles)
    zero = np.zeros_like(cos)
    cos_row = np.concatenate([cos, cos, zero, zero], 1)
    cos_col = np.concatenate([zero, zero, cos, cos], 1)
    sin_row = np.concatenate([-sin, sin, zero, zero], 1)
    sin_col = np.concatenate([zero, zero, -sin, sin], 1)
    table = np.stack([np.stack([cos_row, cos_col]), np.stack([sin_row, sin_col])])
    return np.tile(table, (1, 1, 1, 2)).astype(np.float32)


def silu(v):
    return v / (1.0 + jnp.exp(-v))


def kernel(
    dims,
    latent, context, cond, cctx, gain, msh, msc, mga, qg, kg, vg, lam, lift, rope, wq_h, wk_h, wv_h, wo_h,
    out,
    wq, wk, wv, wo, lat, normed, inv, part, sums, far, full, cosb, sinb, qz, kbuf, vbuf, numer, tot, hosend, ho,
    lsem, p_send, p_recv, f_send, f_recv, c_send, c_recv, y_send, y_recv, w_send, w_recv, r_send, r_recv, o_send, o_recv,
):
    Z, Y = dims
    z, y = lax.axis_index("sp"), lax.axis_index("tp")

    def zz(d):
        return lax.rem(z + (d + Z), Z)

    def yy(d):
        return lax.rem(y + (d + Y), Y)

    loads = [
        pltpu.make_async_copy(wk_h, wk, lsem.at[0]),
        pltpu.make_async_copy(wv_h, wv, lsem.at[1]),
        pltpu.make_async_copy(wq_h, wq, lsem.at[2]),
        pltpu.make_async_copy(wo_h, wo.at[y], lsem.at[3]),
    ]
    for copy in loads:
        copy.start()

    barrier = pltpu.get_barrier_semaphore()
    z_peers = [1, 2, 3, 4, 5, -1, -2, -3, -4, -5]
    for d in z_peers:
        pl.semaphore_signal(barrier, inc=1, device_id={"sp": zz(d)}, device_id_type=MESH)
    for d in (1, 2, 3):
        pl.semaphore_signal(barrier, inc=1, device_id={"tp": yy(d)}, device_id_type=MESH)

    rows16 = lax.broadcasted_iota(jnp.int32, (16, 128), 0)
    a0 = silu(cond[...].astype(F32))
    a1 = silu(cctx[...].astype(F32))
    acts = jnp.where(rows16 == 0, a0, jnp.where(rows16 == 1, a1, 0.0)).astype(BF16)
    p_sh = jnp.dot(acts, msh[...], preferred_element_type=F32)
    p_sc = jnp.dot(acts, msc[...], preferred_element_type=F32)
    p_ga = jnp.dot(acts, mga[...], preferred_element_type=F32)
    part[0, 0:1, :] = p_sh[0:1]
    part[0, 1:2, :] = p_sc[0:1]
    part[0, 2:3, :] = p_ga[0:1]
    part[0, 3:4, :] = p_sh[1:2]
    part[0, 4:5, :] = p_sc[1:2]
    part[0, 5:8, :] = jnp.zeros((3, part.shape[2]), F32)

    pl.semaphore_wait(barrier, len(z_peers) + 3)

    def copy_to(src, dst, ssem, rsem, **where):
        return pltpu.make_async_remote_copy(
            src_ref=src, dst_ref=dst, send_sem=ssem, recv_sem=rsem, device_id=where, device_id_type=MESH
        )

    offs = [-3, 3, -2, 2, -1, 1]
    stage1 = []
    for n, d in enumerate(offs):
        c = copy_to(part.at[0], part.at[n + 1], p_send.at[n], p_recv.at[n], sp=zz(-d))
        c.start()
        stage1.append(c)

    rows = latent.shape[0]
    half = rows // 2
    top, bottom = pl.ds(0, half), pl.ds(half, half)

    def y_copies(src, slots, send, recv, first, second):
        return [
            copy_to(src.at[first], slots.at[y, first], send.at[0], recv.at[0], tp=yy(1)),
            copy_to(src.at[second], slots.at[y, second], send.at[1], recv.at[1], tp=yy(-1)),
            copy_to(src.at[second], slots.at[y, second], send.at[2], recv.at[2], tp=yy(1)),
            copy_to(src.at[first], slots.at[y, first], send.at[3], recv.at[3], tp=yy(-1)),
        ]

    def y_forward(slots, send, recv, first, second):
        return [
            copy_to(slots.at[yy(-1), first], slots.at[yy(-1), first], send.at[4], recv.at[4], tp=yy(1)),
            copy_to(slots.at[yy(1), second], slots.at[yy(1), second], send.at[5], recv.at[5], tp=yy(-1)),
        ]

    lat_sends = y_copies(latent, lat, y_send, y_recv, top, bottom)
    for c in lat_sends:
        c.start()
    lat[y] = latent[...]

    width = wq.shape[1]
    hw = qg.shape[1]
    gi = lax.broadcasted_iota(jnp.int32, (width, width), 0) // hw
    gj = lax.broadcasted_iota(jnp.int32, (width, width), 1) // hw
    average = jnp.where(gi == gj, 1.0 / hw, 0.0).astype(BF16)
    LR = Y * rows
    CR = context.shape[0]
    for k in range(Y):
        at = pl.ds(k * rows, rows)
        cosb[at, :] = rope[0, 0, pl.ds(Y * z + k, 1), :] + rope[0, 1]
        sinb[at, :] = rope[1, 0, pl.ds(Y * z + k, 1), :] + rope[1, 1]
    cosb[pl.ds(LR, CR), :] = jnp.ones((CR, 128), F32)
    sinb[pl.ds(LR, CR), :] = jnp.zeros((CR, 128), F32)

    def mean_square(x):
        xf = x.astype(F32)
        ms = jnp.mean(xf * xf, axis=-1, keepdims=True)
        return jnp.broadcast_to(lax.rsqrt(ms + token_eps), (x.shape[0], 128))

    inv[pl.ds(LR, CR), :] = mean_square(context[...])

    for c in stage1:
        c.wait_recv()
    sums[0] = part[0] + part[5] + part[3] + part[1]
    sums[1] = part[0] + part[6] + part[4] + part[2]
    stage2 = [
        copy_to(sums.at[1], far.at[2], f_send.at[2], f_recv.at[2], sp=zz(-5)),
        copy_to(sums.at[0], far.at[0], f_send.at[0], f_recv.at[0], sp=zz(4)),
        copy_to(sums.at[1], far.at[1], f_send.at[1], f_recv.at[1], sp=zz(-1)),
    ]
    for c in stage2:
        c.start()

    lat_sends[0].wait_recv()
    lat_sends[1].wait_recv()
    lat_forward = y_forward(lat, y_send, y_recv, top, bottom)
    for c in lat_forward:
        c.start()
    inv[pl.ds(y * rows, rows), :] = mean_square(latent[...])
    lat_sends[2].wait_recv()
    lat_sends[3].wait_recv()
    for d in (1, -1):
        inv[pl.ds(yy(d) * rows, rows), :] = mean_square(lat[yy(d)])

    for c in stage2:
        c.wait_recv()
    full[y] = sums[0] + far[0] + far[1] + far[2]
    stage3 = []
    for n, d in enumerate((2, 1, 3)):
        c = copy_to(full.at[y], full.at[y], c_send.at[n], c_recv.at[n], tp=yy(d))
        c.start()
        stage3.append(c)
    for c in lat_forward:
        c.wait_recv()
    inv[pl.ds(yy(2) * rows, rows), :] = mean_square(lat[yy(2)])
    for c in stage3:
        c.wait_recv()

    cb = full.shape[2]
    for b in range(Y):
        cols = pl.ds(b * cb, cb)
        a = gain[:, cols] * (1.0 + full[b, 1:2, :])
        s = full[b, 0:1, :]
        for k in range(Y):
            v = inv[pl.ds(k * rows, rows), :]
            v = jnp.concatenate([v] * (cb // 128), axis=1)
            normed[pl.ds(k * rows, rows), cols] = (lat[k, :, cols].astype(F32) * v * a + s).astype(BF16)
        a = gain[:, cols] * (1.0 + full[b, 4:5, :])
        s = full[b, 3:4, :]
        v = inv[pl.ds(LR, CR), :]
        v = jnp.concatenate([v] * (cb // 128), axis=1)
        normed[pl.ds(LR, CR), cols] = (context[:, cols].astype(F32) * v * a + s).astype(BF16)

    lane = lax.broadcasted_iota(jnp.int32, (1, 128), 1)
    q4 = hw // 4
    is_x = (lane // q4) % 2 == 0

    def head_norm(u, g):
        sq = u * u
        hi = sq.astype(BF16)
        lo = (sq - hi.astype(F32)).astype(BF16)
        ms = jnp.dot(hi, average, preferred_element_type=F32) + jnp.dot(lo, average, preferred_element_type=F32)
        return u * lax.rsqrt(ms + token_eps) * g

    def turn(t, n):
        other = jnp.where(is_x, pltpu.roll(t, 128 - q4, 1), pltpu.roll(t, q4, 1))
        return t * cosb[pl.ds(0, n), :] + other * sinb[pl.ds(0, n), :]

    heads = width // 128
    g2 = jnp.concatenate([kg[...]] * (width // hw), axis=1)
    loads[0].wait()
    u = head_norm(jnp.dot(normed[...], wk[...], preferred_element_type=F32), g2)
    for h in range(heads):
        kbuf[z, :, h * 128 : (h + 1) * 128] = turn(u[:, h * 128 : (h + 1) * 128], LR + CR).astype(BF16)

    def ring(step, direction, which):
        buf = kbuf if which == 0 else vbuf
        slot = lax.rem(z - direction * step + Z, Z)
        to = lax.rem(z + direction + Z, Z)
        side = 0 if direction == 1 else 1
        return copy_to(
            buf.at[slot], buf.at[slot], r_send.at[side, which, step], r_recv.at[side, which, step], sp=to
        )

    for direction in (1, -1):
        ring(0, direction, 0).start()
    loads[1].wait()
    vbuf[z] = jnp.dot(normed[...], wv[...], preferred_element_type=F32).astype(BF16)
    for direction in (1, -1):
        ring(0, direction, 1).start()

    loads[2].wait()
    g2 = jnp.concatenate([qg[...]] * (width // hw), axis=1)
    u = head_norm(jnp.dot(normed[pl.ds(0, LR), :], wq[...], preferred_element_type=F32), g2)
    for h in range(heads):
        t = turn(u[:, h * 128 : (h + 1) * 128], LR) * (hw ** -0.5)
        qz[h, pl.ds(0, LR), :] = jnp.where(lane < hw, t, 0.0).astype(BF16)
        qz[h, pl.ds(LR, LR), :] = jnp.where(lane < hw, 0.0, t).astype(BF16)

    wh = wo.shape[1] // 2
    loads[3].wait()
    wo_sends = y_copies(wo.at[y], wo, w_send, w_recv, pl.ds(0, wh), pl.ds(wh, wh))
    for c in wo_sends:
        c.start()

    numer[...] = jnp.zeros_like(numer)
    tot[...] = jnp.zeros_like(tot)

    def attend(h, keys, values, extra):
        s = lax.dot_general(qz[h], keys, (((1,), (1,)), ((), ())), preferred_element_type=F32)
        if extra is not None:
            s = s + extra
        w = jnp.exp(s)
        t = w[:, 0:128]
        for j in range(1, w.shape[1] // 128):
            t = t + w[:, j * 128 : (j + 1) * 128]
        tot[h] = tot[h] + t
        numer[h] = numer[h] + jnp.dot(w.astype(BF16), values, preferred_element_type=F32)

    def attend_slot(slot):
        def one(h, carry):
            hc = pl.ds(pl.multiple_of(h * 128, 128), 128)
            attend(h, kbuf[slot, pl.ds(0, LR), hc], vbuf[slot, pl.ds(0, LR), hc], None)
            return carry

        lax.fori_loop(0, heads, one, 0)

    attend_slot(z)
    last = Z // 2

    def hop(s, carry):
        for which in (0, 1):
            for direction in (1, -1):
                ring(s - 1, direction, which).wait_recv()
                ring(s, direction, which).start()
        attend_slot(lax.rem(z - s + Z, Z))
        attend_slot(lax.rem(z + s, Z))
        return carry

    mid = last // 2
    lax.fori_loop(1, mid, hop, 0)
    wo_sends[0].wait_recv()
    wo_sends[1].wait_recv()
    wo_forward = y_forward(wo, w_send, w_recv, pl.ds(0, wh), pl.ds(wh, wh))
    for c in wo_forward:
        c.start()
    lax.fori_loop(mid, last - 1, hop, 0)
    s = last - 1
    for direction in (1, -1):
        ring(s - 1, direction, 0).wait_recv()
        if direction == 1:
            ring(s, direction, 0).start()
    for direction in (1, -1):
        ring(s - 1, direction, 1).wait_recv()
        if direction == -1:
            ring(s, direction, 1).start()
    attend_slot(lax.rem(z - s + Z, Z))
    attend_slot(lax.rem(z + s, Z))
    ring(s, 1, 0).wait_recv()
    ring(s, -1, 1).wait_recv()
    attend_slot(lax.rem(z + last, Z))

    for h in range(heads):
        hc = slice(h * 128, (h + 1) * 128)
        keys = kbuf[:, pl.ds(LR, CR), hc].reshape(Z * CR, 128)
        values = vbuf[:, pl.ds(LR, CR), hc].reshape(Z * CR, 128)
        attend(h, keys, values, lift[h])

    for h in range(heads):
        total = jnp.sum(tot[h], axis=-1, keepdims=True)
        ratio = numer[h] / total
        mixed = ratio[0:LR] - lam[h] * ratio[LR : 2 * LR]
        ms = jnp.mean(mixed * mixed, axis=-1, keepdims=True)
        res = (mixed * lax.rsqrt(ms + head_eps) * vg[...] * head_factor).astype(BF16)
        for k in range(Y):
            hosend[k, :, h * 128 : (h + 1) * 128] = res[k * rows : (k + 1) * rows]
    o_copies = []
    for n, d in enumerate((2, 1, 3)):
        c = copy_to(hosend.at[yy(d)], ho.at[y], o_send.at[n], o_recv.at[n], tp=yy(d))
        c.start()
        o_copies.append(c)
    ho[y] = hosend[y]
    for c in wo_sends[2:] + wo_forward:
        c.wait_recv()
    for c in o_copies:
        c.wait_recv()
    for b in range(Y):
        cols = pl.ds(b * cb, cb)
        acc = jnp.zeros((rows, cb), F32)
        for k in range(Y):
            acc = acc + jnp.dot(ho[k], wo[k, :, cols], preferred_element_type=F32)
        out[:, cols] = (latent[:, cols].astype(F32) + full[b, 2:3, :] * acc).astype(BF16)

    for c in stage1 + stage2 + stage3 + lat_sends + lat_forward + wo_sends + wo_forward + o_copies:
        c.wait_send()
    for s in range(last - 1):
        for direction in (1, -1):
            for which in (0, 1):
                ring(s, direction, which).wait_send()
    ring(last - 1, 1, 0).wait_send()
    ring(last - 1, -1, 1).wait_send()


def on_device(
    sizes, latent, context, cond, context_cond, norm_gain, mod_shift, mod_scale, mod_gate, w_query, w_key, w_value,
    query_gain, key_gain, mix_lambda, context_lift, value_gain, w_out,
):
    Z, Y = sizes
    rows, D = latent.shape
    cr = context.shape[0]
    LR = Y * rows
    width = w_query.shape[1]
    heads = width // 128
    cb = mod_shift.shape[1]
    rope = jnp.asarray(rope_table(query_gain.shape[0]))
    vmem = pl.BlockSpec(memory_space=pltpu.VMEM)
    smem = pl.BlockSpec(memory_space=pltpu.SMEM)
    anys = pl.BlockSpec(memory_space=pl.ANY)
    dma = pltpu.SemaphoreType.DMA
    V = pltpu.VMEM
    return pl.pallas_call(
        functools.partial(kernel, sizes),
        out_shape=jax.ShapeDtypeStruct((rows, D), BF16),
        in_specs=[vmem] * 11 + [smem] * 2 + [vmem] + [anys] * 4,
        out_specs=vmem,
        scratch_shapes=[
            V((D, width), BF16), V((D, width), BF16), V((D, width), BF16), V((Y, w_out.shape[0], D), BF16),
            V((Y, rows, D), BF16), V((LR + cr, D), BF16), V((LR + cr, 128), F32),
            V((7, 8, cb), F32), V((2, 8, cb), F32), V((3, 8, cb), F32), V((Y, 8, cb), F32),
            V((LR + cr, 128), F32), V((LR + cr, 128), F32),
            V((heads, 2 * LR, 128), BF16), V((Z, LR + cr, width), BF16), V((Z, LR + cr, width), BF16),
            V((heads, 2 * LR, 128), F32), V((heads, 2 * LR, 128), F32),
            V((Y, rows, width), BF16), V((Y, rows, width), BF16),
            dma((4,)), dma((6,)), dma((6,)), dma((3,)), dma((3,)), dma((3,)), dma((3,)), dma((6,)), dma((6,)),
            dma((6,)), dma((6,)), dma((2, 2, Z // 2)), dma((2, 2, Z // 2)), dma((3,)), dma((3,)),
        ],
        compiler_params=pltpu.CompilerParams(
            collective_id=0, has_side_effects=True, vmem_limit_bytes=48 * 1024 * 1024
        ),
    )(
        latent, context, cond.reshape(1, -1), context_cond.reshape(1, -1), norm_gain.reshape(1, -1),
        mod_shift, mod_scale, mod_gate, query_gain.reshape(1, -1), key_gain.reshape(1, -1), value_gain.reshape(1, -1),
        mix_lambda, context_lift, rope, w_query, w_key, w_value, w_out,
    )


def solution(mesh):
    placed = (
        P(("dp", "sp", "tp"), None),
        P(("dp", "sp"), None),
        P(("dp", "sp")),
        P("sp"),
        P(),
        P("sp", "tp"),
        P("sp", "tp"),
        P("sp", "tp"),
        P(None, "tp"),
        P(None, "tp"),
        P(None, "tp"),
        P(),
        P(),
        P("tp"),
        P("tp"),
        P(),
        P("tp", None),
    )
    sizes = (mesh.shape["sp"], mesh.shape["tp"])
    return jax.shard_map(
        functools.partial(on_device, sizes),
        mesh=mesh,
        in_specs=placed,
        out_specs=P(("dp", "sp", "tp"), None),
        check_vma=False,
    )
```

```python
import functools

import jax
import jax.numpy as jnp
import numpy as np
from jax import lax
from jax.experimental import pallas as pl
from jax.experimental.pallas import tpu as pltpu
from jax.sharding import PartitionSpec as P

GRID = 64
token_eps = 0.01
head_eps = 0.001
rope_base = 10000.0
head_factor = 0.8
MESH = pl.DeviceIdType.MESH
F32 = jnp.float32
BF16 = jnp.bfloat16


def rope_table(head_width):
    quarter = head_width // 4
    inverse = np.float32(rope_base) ** (-np.arange(quarter, dtype=np.float32) / np.float32(quarter))
    angles = (np.arange(GRID, dtype=np.float32)[:, None] * inverse).astype(np.float64)
    cos, sin = np.cos(angles), np.sin(angles)
    zero = np.zeros_like(cos)
    cos_row = np.concatenate([cos, cos, zero, zero], 1)
    cos_col = np.concatenate([zero, zero, cos, cos], 1)
    sin_row = np.concatenate([-sin, sin, zero, zero], 1)
    sin_col = np.concatenate([zero, zero, -sin, sin], 1)
    table = np.stack([np.stack([cos_row, cos_col]), np.stack([sin_row, sin_col])])
    return np.tile(table, (1, 1, 1, 2)).astype(np.float32)


def silu(v):
    return v / (1.0 + jnp.exp(-v))


def kernel(
    dims,
    latent, context, cond, cctx, gain, msh, msc, mga, qg, kg, vg, lam, lift, rope, wq_h, wk_h, wv_h, wo_h,
    out,
    wq, wk, wv, wo, lat, normed, inv, part, sums, far, full, cosb, sinb, qz, kbuf, vbuf, numer, tot, hosend, ho,
    lsem, p_send, p_recv, f_send, f_recv, c_send, c_recv, y_send, y_recv, w_send, w_recv, r_send, r_recv, o_send, o_recv,
):
    Z, Y = dims
    z, y = lax.axis_index("sp"), lax.axis_index("tp")

    def zz(d):
        return lax.rem(z + (d + Z), Z)

    def yy(d):
        return lax.rem(y + (d + Y), Y)

    loads = [
        pltpu.make_async_copy(wk_h, wk, lsem.at[0]),
        pltpu.make_async_copy(wv_h, wv, lsem.at[1]),
        pltpu.make_async_copy(wq_h, wq, lsem.at[2]),
        pltpu.make_async_copy(wo_h, wo.at[y], lsem.at[3]),
    ]
    for copy in loads:
        copy.start()

    barrier = pltpu.get_barrier_semaphore()
    z_peers = [1, 2, 3, 4, 5, -1, -2, -3, -4, -5]
    for d in z_peers:
        pl.semaphore_signal(barrier, inc=1, device_id={"sp": zz(d)}, device_id_type=MESH)
    for d in (1, 2, 3):
        pl.semaphore_signal(barrier, inc=1, device_id={"tp": yy(d)}, device_id_type=MESH)

    rows16 = lax.broadcasted_iota(jnp.int32, (16, 128), 0)
    a0 = silu(cond[...].astype(F32))
    a1 = silu(cctx[...].astype(F32))
    acts = jnp.where(rows16 == 0, a0, jnp.where(rows16 == 1, a1, 0.0)).astype(BF16)
    p_sh = jnp.dot(acts, msh[...], preferred_element_type=F32)
    p_sc = jnp.dot(acts, msc[...], preferred_element_type=F32)
    p_ga = jnp.dot(acts, mga[...], preferred_element_type=F32)
    part[0, 0:1, :] = p_sh[0:1]
    part[0, 1:2, :] = p_sc[0:1]
    part[0, 2:3, :] = p_ga[0:1]
    part[0, 3:4, :] = p_sh[1:2]
    part[0, 4:5, :] = p_sc[1:2]
    part[0, 5:8, :] = jnp.zeros((3, part.shape[2]), F32)

    pl.semaphore_wait(barrier, len(z_peers) + 3)

    def copy_to(src, dst, ssem, rsem, **where):
        return pltpu.make_async_remote_copy(
            src_ref=src, dst_ref=dst, send_sem=ssem, recv_sem=rsem, device_id=where, device_id_type=MESH
        )

    offs = [-3, 3, -2, 2, -1, 1]
    stage1 = []
    for n, d in enumerate(offs):
        c = copy_to(part.at[0], part.at[n + 1], p_send.at[n], p_recv.at[n], sp=zz(-d))
        c.start()
        stage1.append(c)

    rows = latent.shape[0]
    half = rows // 2
    top, bottom = pl.ds(0, half), pl.ds(half, half)

    def y_copies(src, slots, send, recv, first, second):
        return [
            copy_to(src.at[first], slots.at[y, first], send.at[0], recv.at[0], tp=yy(1)),
            copy_to(src.at[second], slots.at[y, second], send.at[1], recv.at[1], tp=yy(-1)),
            copy_to(src.at[second], slots.at[y, second], send.at[2], recv.at[2], tp=yy(1)),
            copy_to(src.at[first], slots.at[y, first], send.at[3], recv.at[3], tp=yy(-1)),
        ]

    def y_forward(slots, send, recv, first, second):
        return [
            copy_to(slots.at[yy(-1), first], slots.at[yy(-1), first], send.at[4], recv.at[4], tp=yy(1)),
            copy_to(slots.at[yy(1), second], slots.at[yy(1), second], send.at[5], recv.at[5], tp=yy(-1)),
        ]

    lat_sends = y_copies(latent, lat, y_send, y_recv, top, bottom)
    for c in lat_sends:
        c.start()
    lat[y] = latent[...]

    width = wq.shape[1]
    hw = qg.shape[1]
    gi = lax.broadcasted_iota(jnp.int32, (width, width), 0) // hw
    gj = lax.broadcasted_iota(jnp.int32, (width, width), 1) // hw
    average = jnp.where(gi == gj, 1.0 / hw, 0.0).astype(BF16)
    LR = Y * rows
    CR = context.shape[0]
    for k in range(Y):
        at = pl.ds(k * rows, rows)
        cosb[at, :] = rope[0, 0, pl.ds(Y * z + k, 1), :] + rope[0, 1]
        sinb[at, :] = rope[1, 0, pl.ds(Y * z + k, 1), :] + rope[1, 1]
    cosb[pl.ds(LR, CR), :] = jnp.ones((CR, 128), F32)
    sinb[pl.ds(LR, CR), :] = jnp.zeros((CR, 128), F32)

    def mean_square(x):
        xf = x.astype(F32)
        ms = jnp.mean(xf * xf, axis=-1, keepdims=True)
        return jnp.broadcast_to(lax.rsqrt(ms + token_eps), (x.shape[0], 128))

    inv[pl.ds(LR, CR), :] = mean_square(context[...])

    for c in stage1:
        c.wait_recv()
    sums[0] = part[0] + part[5] + part[3] + part[1]
    sums[1] = part[0] + part[6] + part[4] + part[2]
    stage2 = [
        copy_to(sums.at[1], far.at[2], f_send.at[2], f_recv.at[2], sp=zz(-5)),
        copy_to(sums.at[0], far.at[0], f_send.at[0], f_recv.at[0], sp=zz(4)),
        copy_to(sums.at[1], far.at[1], f_send.at[1], f_recv.at[1], sp=zz(-1)),
    ]
    for c in stage2:
        c.start()

    lat_sends[0].wait_recv()
    lat_sends[1].wait_recv()
    lat_forward = y_forward(lat, y_send, y_recv, top, bottom)
    for c in lat_forward:
        c.start()
    inv[pl.ds(y * rows, rows), :] = mean_square(latent[...])
    lat_sends[2].wait_recv()
    lat_sends[3].wait_recv()
    for d in (1, -1):
        inv[pl.ds(yy(d) * rows, rows), :] = mean_square(lat[yy(d)])

    for c in stage2:
        c.wait_recv()
    full[y] = sums[0] + far[0] + far[1] + far[2]
    stage3 = []
    for n, d in enumerate((2, 1, 3)):
        c = copy_to(full.at[y], full.at[y], c_send.at[n], c_recv.at[n], tp=yy(d))
        c.start()
        stage3.append(c)
    for c in lat_forward:
        c.wait_recv()
    inv[pl.ds(yy(2) * rows, rows), :] = mean_square(lat[yy(2)])
    for c in stage3:
        c.wait_recv()

    cb = full.shape[2]
    for b in range(Y):
        cols = pl.ds(b * cb, cb)
        a = gain[:, cols] * (1.0 + full[b, 1:2, :])
        s = full[b, 0:1, :]
        for k in range(Y):
            v = inv[pl.ds(k * rows, rows), :]
            v = jnp.concatenate([v] * (cb // 128), axis=1)
            normed[pl.ds(k * rows, rows), cols] = (lat[k, :, cols].astype(F32) * v * a + s).astype(BF16)
        a = gain[:, cols] * (1.0 + full[b, 4:5, :])
        s = full[b, 3:4, :]
        v = inv[pl.ds(LR, CR), :]
        v = jnp.concatenate([v] * (cb // 128), axis=1)
        normed[pl.ds(LR, CR), cols] = (context[:, cols].astype(F32) * v * a + s).astype(BF16)

    lane = lax.broadcasted_iota(jnp.int32, (1, 128), 1)
    q4 = hw // 4
    is_x = (lane // q4) % 2 == 0

    def head_norm(u, g):
        sq = u * u
        hi = sq.astype(BF16)
        lo = (sq - hi.astype(F32)).astype(BF16)
        ms = jnp.dot(hi, average, preferred_element_type=F32) + jnp.dot(lo, average, preferred_element_type=F32)
        return u * lax.rsqrt(ms + token_eps) * g

    def turn(t, n):
        other = jnp.where(is_x, pltpu.roll(t, 128 - q4, 1), pltpu.roll(t, q4, 1))
        return t * cosb[pl.ds(0, n), :] + other * sinb[pl.ds(0, n), :]

    heads = width // 128
    g2 = jnp.concatenate([kg[...]] * (width // hw), axis=1)
    loads[0].wait()
    u = head_norm(jnp.dot(normed[...], wk[...], preferred_element_type=F32), g2)
    for h in range(heads):
        kbuf[z, :, h * 128 : (h + 1) * 128] = turn(u[:, h * 128 : (h + 1) * 128], LR + CR).astype(BF16)

    def ring(step, direction, which):
        buf = kbuf if which == 0 else vbuf
        slot = lax.rem(z - direction * step + Z, Z)
        to = lax.rem(z + direction + Z, Z)
        side = 0 if direction == 1 else 1
        return copy_to(
            buf.at[slot], buf.at[slot], r_send.at[side, which, step], r_recv.at[side, which, step], sp=to
        )

    for direction in (1, -1):
        ring(0, direction, 0).start()
    loads[1].wait()
    vbuf[z] = jnp.dot(normed[...], wv[...], preferred_element_type=F32).astype(BF16)
    for direction in (1, -1):
        ring(0, direction, 1).start()

    loads[2].wait()
    g2 = jnp.concatenate([qg[...]] * (width // hw), axis=1)
    u = head_norm(jnp.dot(normed[pl.ds(0, LR), :], wq[...], preferred_element_type=F32), g2)
    for h in range(heads):
        t = turn(u[:, h * 128 : (h + 1) * 128], LR) * (hw ** -0.5)
        qz[h, pl.ds(0, LR), :] = jnp.where(lane < hw, t, 0.0).astype(BF16)
        qz[h, pl.ds(LR, LR), :] = jnp.where(lane < hw, 0.0, t).astype(BF16)

    wh = wo.shape[1] // 2
    loads[3].wait()
    wo_sends = y_copies(wo.at[y], wo, w_send, w_recv, pl.ds(0, wh), pl.ds(wh, wh))
    for c in wo_sends:
        c.start()

    numer[...] = jnp.zeros_like(numer)
    tot[...] = jnp.zeros_like(tot)

    def attend(h, keys, values, extra):
        s = lax.dot_general(qz[h], keys, (((1,), (1,)), ((), ())), preferred_element_type=F32)
        if extra is not None:
            s = s + extra
        w = jnp.exp(s)
        t = w[:, 0:128]
        for j in range(1, w.shape[1] // 128):
            t = t + w[:, j * 128 : (j + 1) * 128]
        tot[h] = tot[h] + t
        numer[h] = numer[h] + jnp.dot(w.astype(BF16), values, preferred_element_type=F32)

    def attend_slot(slot):
        def one(h, carry):
            hc = pl.ds(pl.multiple_of(h * 128, 128), 128)
            attend(h, kbuf[slot, pl.ds(0, LR), hc], vbuf[slot, pl.ds(0, LR), hc], None)
            return carry

        lax.fori_loop(0, heads, one, 0)

    attend_slot(z)
    last = Z // 2

    def hop(s, carry):
        for which in (0, 1):
            for direction in (1, -1):
                ring(s - 1, direction, which).wait_recv()
                ring(s, direction, which).start()
        attend_slot(lax.rem(z - s + Z, Z))
        attend_slot(lax.rem(z + s, Z))
        return carry

    mid = last // 2
    lax.fori_loop(1, mid, hop, 0)
    wo_sends[0].wait_recv()
    wo_sends[1].wait_recv()
    wo_forward = y_forward(wo, w_send, w_recv, pl.ds(0, wh), pl.ds(wh, wh))
    for c in wo_forward:
        c.start()
    lax.fori_loop(mid, last - 1, hop, 0)
    s = last - 1
    for direction in (1, -1):
        ring(s - 1, direction, 0).wait_recv()
        if direction == 1:
            ring(s, direction, 0).start()
    for direction in (1, -1):
        ring(s - 1, direction, 1).wait_recv()
        if direction == -1:
            ring(s, direction, 1).start()
    attend_slot(lax.rem(z - s + Z, Z))
    attend_slot(lax.rem(z + s, Z))
    ring(s, 1, 0).wait_recv()
    ring(s, -1, 1).wait_recv()
    attend_slot(lax.rem(z + last, Z))

    for h in range(heads):
        hc = slice(h * 128, (h + 1) * 128)
        keys = kbuf[:, pl.ds(LR, CR), hc].reshape(Z * CR, 128)
        values = vbuf[:, pl.ds(LR, CR), hc].reshape(Z * CR, 128)
        attend(h, keys, values, lift[h])

    for h in range(heads):
        total = jnp.sum(tot[h], axis=-1, keepdims=True)
        ratio = numer[h] / total
        mixed = ratio[0:LR] - lam[h] * ratio[LR : 2 * LR]
        ms = jnp.mean(mixed * mixed, axis=-1, keepdims=True)
        res = (mixed * lax.rsqrt(ms + head_eps) * vg[...] * head_factor).astype(BF16)
        for k in range(Y):
            hosend[k, :, h * 128 : (h + 1) * 128] = res[k * rows : (k + 1) * rows]
    o_copies = []
    for n, d in enumerate((2, 1, 3)):
        c = copy_to(hosend.at[yy(d)], ho.at[y], o_send.at[n], o_recv.at[n], tp=yy(d))
        c.start()
        o_copies.append(c)
    ho[y] = hosend[y]
    for c in wo_sends[2:] + wo_forward:
        c.wait_recv()
    for c in o_copies:
        c.wait_recv()
    for b in range(Y):
        cols = pl.ds(b * cb, cb)
        acc = jnp.zeros((rows, cb), F32)
        for k in range(Y):
            acc = acc + jnp.dot(ho[k], wo[k, :, cols], preferred_element_type=F32)
        out[:, cols] = (latent[:, cols].astype(F32) + full[b, 2:3, :] * acc).astype(BF16)

    for c in stage1 + stage2 + stage3 + lat_sends + lat_forward + wo_sends + wo_forward + o_copies:
        c.wait_send()
    for s in range(last - 1):
        for direction in (1, -1):
            for which in (0, 1):
                ring(s, direction, which).wait_send()
    ring(last - 1, 1, 0).wait_send()
    ring(last - 1, -1, 1).wait_send()


def on_device(
    sizes, latent, context, cond, context_cond, norm_gain, mod_shift, mod_scale, mod_gate, w_query, w_key, w_value,
    query_gain, key_gain, mix_lambda, context_lift, value_gain, w_out,
):
    Z, Y = sizes
    rows, D = latent.shape
    cr = context.shape[0]
    LR = Y * rows
    width = w_query.shape[1]
    heads = width // 128
    cb = mod_shift.shape[1]
    rope = jnp.asarray(rope_table(query_gain.shape[0]))
    vmem = pl.BlockSpec(memory_space=pltpu.VMEM)
    smem = pl.BlockSpec(memory_space=pltpu.SMEM)
    anys = pl.BlockSpec(memory_space=pl.ANY)
    dma = pltpu.SemaphoreType.DMA
    V = pltpu.VMEM
    return pl.pallas_call(
        functools.partial(kernel, sizes),
        out_shape=jax.ShapeDtypeStruct((rows, D), BF16),
        in_specs=[vmem] * 11 + [smem] * 2 + [vmem] + [anys] * 4,
        out_specs=vmem,
        scratch_shapes=[
            V((D, width), BF16), V((D, width), BF16), V((D, width), BF16), V((Y, w_out.shape[0], D), BF16),
            V((Y, rows, D), BF16), V((LR + cr, D), BF16), V((LR + cr, 128), F32),
            V((7, 8, cb), F32), V((2, 8, cb), F32), V((3, 8, cb), F32), V((Y, 8, cb), F32),
            V((LR + cr, 128), F32), V((LR + cr, 128), F32),
            V((heads, 2 * LR, 128), BF16), V((Z, LR + cr, width), BF16), V((Z, LR + cr, width), BF16),
            V((heads, 2 * LR, 128), F32), V((heads, 2 * LR, 128), F32),
            V((Y, rows, width), BF16), V((Y, rows, width), BF16),
            dma((4,)), dma((6,)), dma((6,)), dma((3,)), dma((3,)), dma((3,)), dma((3,)), dma((6,)), dma((6,)),
            dma((6,)), dma((6,)), dma((2, 2, Z // 2)), dma((2, 2, Z // 2)), dma((3,)), dma((3,)),
        ],
        compiler_params=pltpu.CompilerParams(
            collective_id=0, has_side_effects=True, vmem_limit_bytes=67043328
        ),
    )(
        latent, context, cond.reshape(1, -1), context_cond.reshape(1, -1), norm_gain.reshape(1, -1),
        mod_shift, mod_scale, mod_gate, query_gain.reshape(1, -1), key_gain.reshape(1, -1), value_gain.reshape(1, -1),
        mix_lambda, context_lift, rope, w_query, w_key, w_value, w_out,
    )


def solution(mesh):
    placed = (
        P(("dp", "sp", "tp"), None),
        P(("dp", "sp"), None),
        P(("dp", "sp")),
        P("sp"),
        P(),
        P("sp", "tp"),
        P("sp", "tp"),
        P("sp", "tp"),
        P(None, "tp"),
        P(None, "tp"),
        P(None, "tp"),
        P(),
        P(),
        P("tp"),
        P("tp"),
        P(),
        P("tp", None),
    )
    sizes = (mesh.shape["sp"], mesh.shape["tp"])
    return jax.shard_map(
        functools.partial(on_device, sizes),
        mesh=mesh,
        in_specs=placed,
        out_specs=P(("dp", "sp", "tp"), None),
        check_vma=False,
    )
```

```python
import functools

import jax
import jax.numpy as jnp
import numpy as np
from jax import lax
from jax.experimental import pallas as pl
from jax.experimental.pallas import tpu as pltpu
from jax.sharding import PartitionSpec as P

GRID = 64
token_eps = 0.01
head_eps = 0.001
rope_base = 10000.0
head_factor = 0.8
MESH = pl.DeviceIdType.MESH
F32 = jnp.float32
BF16 = jnp.bfloat16


def rope_table(head_width):
    quarter = head_width // 4
    inverse = np.float32(rope_base) ** (-np.arange(quarter, dtype=np.float32) / np.float32(quarter))
    angles = (np.arange(GRID, dtype=np.float32)[:, None] * inverse).astype(np.float64)
    cos, sin = np.cos(angles), np.sin(angles)
    zero = np.zeros_like(cos)
    cos_row = np.concatenate([cos, cos, zero, zero], 1)
    cos_col = np.concatenate([zero, zero, cos, cos], 1)
    sin_row = np.concatenate([-sin, sin, zero, zero], 1)
    sin_col = np.concatenate([zero, zero, -sin, sin], 1)
    table = np.stack([np.stack([cos_row, cos_col]), np.stack([sin_row, sin_col])])
    return np.tile(table, (1, 1, 1, 2)).astype(np.float32)


def silu(v):
    return v / (1.0 + jnp.exp(-v))


def kernel(
    dims,
    latent_h, context_h, cond_h, cctx_h, gain_h, msh_h, msc_h, mga_h, qg_h, kg_h, vg_h, lam_h, lift_h, rope_h,
    wk_h, wv_h, wq_h, wo_h,
    out,
    latent, context, cond, cctx, gain, msh, msc, mga, qg, kg, vg, lam, lift, rope, wk, wv, wq,
    wo, lat, xi, xc, accs, oacc, part, sums, far, full, partn, sumsn, farn, fulln, cosb, sinb, qz, kbuf, vbuf, cbuf,
    numer, tot, hosend, ho,
    lsem, p_send, p_recv, f_send, f_recv, c_send, c_recv, y_send, y_recv, w_send, w_recv, r_send, r_recv, o_send, o_recv,
):
    Z, Y = dims
    z, y = lax.axis_index("sp"), lax.axis_index("tp")

    def zz(d):
        return lax.rem(z + (d + Z), Z)

    def yy(d):
        return lax.rem(y + (d + Y), Y)

    barrier = pltpu.get_barrier_semaphore()
    z_peers = [4, -4, 3, -3, 2, -2, 1, -1]
    for d in z_peers:
        pl.semaphore_signal(barrier, inc=1, device_id={"sp": zz(d)}, device_id_type=MESH)
    for d in (2, 1, 3):
        pl.semaphore_signal(barrier, inc=1, device_id={"tp": yy(d)}, device_id_type=MESH)

    pairs = [
        (cond_h, cond), (cctx_h, cctx), (msh_h, msh), (msc_h, msc), (mga_h, mga), (latent_h, latent), (rope_h, rope),
        (gain_h, gain), (context_h, context), (qg_h, qg), (kg_h, kg), (vg_h, vg), (lam_h, lam), (lift_h, lift),
        (wv_h, wv), (wk_h, wk), (wq_h, wq), (wo_h, wo.at[y]),
    ]
    loads = [pltpu.make_async_copy(src, dst, lsem.at[n]) for n, (src, dst) in enumerate(pairs)]
    for copy in loads:
        copy.start()
    for copy in loads[:5]:
        copy.wait()

    rows16 = lax.broadcasted_iota(jnp.int32, (16, 128), 0)
    a0 = silu(cond[...].astype(F32))
    a1 = silu(cctx[...].astype(F32))
    acts = jnp.where(rows16 == 0, a0, jnp.where(rows16 == 1, a1, 0.0)).astype(BF16)
    p_sh = jnp.dot(acts, msh[...], preferred_element_type=F32)
    p_sc = jnp.dot(acts, msc[...], preferred_element_type=F32)
    p_ga = jnp.dot(acts, mga[...], preferred_element_type=F32)
    T = msh.shape[1] // 128
    for j in range(T):
        js = slice(j * 128, (j + 1) * 128)
        part[0, j : j + 1, :] = p_sh[0:1, js]
        part[0, T + j : T + j + 1, :] = p_sc[0:1, js]
        partn[0, j : j + 1, :] = p_ga[0:1, js]
        partn[0, T + j : T + j + 1, :] = p_sh[1:2, js]
        partn[0, 2 * T + j : 2 * T + j + 1, :] = p_sc[1:2, js]
        partn[0, 3 * T + j : 3 * T + j + 1, :] = jnp.zeros((1, 128), F32)
    loads[5].wait()

    pl.semaphore_wait(barrier, len(z_peers) + 3)

    def copy_to(src, dst, ssem, rsem, **where):
        return pltpu.make_async_remote_copy(
            src_ref=src, dst_ref=dst, send_sem=ssem, recv_sem=rsem, device_id=where, device_id_type=MESH
        )

    offs = [-4, 3, -3, 2, -2, 1, -1]

    def first_stage(buf, g):
        return [
            copy_to(buf.at[0], buf.at[n + 1], p_send.at[g, n], p_recv.at[g, n], sp=zz(-d)) for n, d in enumerate(offs)
        ]

    stage1 = first_stage(part, 0)
    stage1n = first_stage(partn, 1)
    for c in stage1:
        c.start()

    rows = latent.shape[0]
    half = rows // 2
    top, bottom = pl.ds(0, half), pl.ds(half, half)

    def y_copies(src, slots, send, recv, first, second):
        return [
            copy_to(src.at[first], slots.at[y, first], send.at[0], recv.at[0], tp=yy(1)),
            copy_to(src.at[second], slots.at[y, second], send.at[1], recv.at[1], tp=yy(-1)),
            copy_to(src.at[second], slots.at[y, second], send.at[2], recv.at[2], tp=yy(1)),
            copy_to(src.at[first], slots.at[y, first], send.at[3], recv.at[3], tp=yy(-1)),
        ]

    def y_forward(slots, send, recv, first, second):
        return [
            copy_to(slots.at[yy(-1), first], slots.at[yy(-1), first], send.at[4], recv.at[4], tp=yy(1)),
            copy_to(slots.at[yy(1), second], slots.at[yy(1), second], send.at[5], recv.at[5], tp=yy(-1)),
        ]

    lat_sends = y_copies(latent, lat, y_send, y_recv, top, bottom)
    for c in lat_sends:
        c.start()
    for c in stage1n:
        c.start()

    def unit(x):
        xf = x.astype(F32)
        return xf * lax.rsqrt(jnp.mean(xf * xf, axis=-1, keepdims=True) + token_eps)

    width = wq.shape[1]
    hw = qg.shape[1]
    LR = Y * rows
    CR = context.shape[0]
    xi[y] = unit(latent[...])

    def window(buf):
        t = buf[0]
        for n in range(len(offs)):
            t = t + buf[n + 1]
        return t

    def second_stage(src, dst, g):
        return [
            copy_to(src, dst.at[n], f_send.at[g, n], f_recv.at[g, n], sp=zz(d)) for n, d in enumerate((4, -4))
        ]

    for c in stage1:
        c.wait_recv()
    sums[...] = window(part)
    stage2 = second_stage(sums, far, 0)
    for c in stage2:
        c.start()
    for c in stage1n:
        c.wait_recv()
    sumsn[...] = window(partn)
    stage2n = second_stage(sumsn, farn, 1)
    for c in stage2n:
        c.start()

    lat_sends[0].wait_recv()
    lat_sends[1].wait_recv()
    lat_forward = y_forward(lat, y_send, y_recv, top, bottom)
    for c in lat_forward:
        c.start()

    gi = lax.broadcasted_iota(jnp.int32, (width, width), 0) // hw
    gj = lax.broadcasted_iota(jnp.int32, (width, width), 1) // hw
    average = jnp.where(gi == gj, 1.0 / hw, 0.0).astype(BF16)
    for copy in loads[6:14]:
        copy.wait()
    for k in range(Y):
        at = pl.ds(k * rows, rows)
        cosb[at, :] = rope[0, 0, pl.ds(Y * z + k, 1), :] + rope[0, 1]
        sinb[at, :] = rope[1, 0, pl.ds(Y * z + k, 1), :] + rope[1, 1]
    xc[...] = unit(context[...])
    lat_sends[2].wait_recv()
    lat_sends[3].wait_recv()
    for d in (1, -1):
        xi[yy(d)] = unit(lat[yy(d)])

    def third_stage(buf, g):
        return [
            copy_to(buf.at[y], buf.at[y], c_send.at[g, n], c_recv.at[g, n], tp=yy(d)) for n, d in enumerate((2, 1, 3))
        ]

    for c in stage2:
        c.wait_recv()
    full[y] = far[0] + far[1]
    stage3 = third_stage(full, 0)
    for c in stage3:
        c.start()
    for c in lat_forward:
        c.wait_recv()
    xi[yy(2)] = unit(lat[yy(2)])
    for copy in loads[14:17]:
        copy.wait()

    cb = T * 128

    def row_of(buf, b, r):
        return jnp.concatenate([buf[b, r * T + j : r * T + j + 1, :] for j in range(T)], axis=1)

    def columns(b):
        return pl.ds(pl.multiple_of(b * cb, cb), cb)

    def modulated(b):
        at = columns(b)
        scaled = gain[:, at] * (1.0 + row_of(full, b, 1))
        return (xi[:, :, at].reshape(LR, cb) * scaled + row_of(full, b, 0)).astype(BF16)

    def product(part_rows, weight, b):
        return jnp.dot(part_rows, weight[columns(b), :], preferred_element_type=F32)

    block = modulated(y)
    for n, weight in enumerate((wv, wk, wq)):
        accs[n] = product(block, weight, y)
    for m, d in ((2, -3), (1, -1)):
        stage3[m].wait_recv()
        block = modulated(yy(d))
        for n, weight in enumerate((wv, wk, wq)):
            accs[n] = accs[n] + product(block, weight, yy(d))
    stage3[0].wait_recv()
    block = modulated(yy(2))

    lane = lax.broadcasted_iota(jnp.int32, (1, 128), 1)
    q4 = hw // 4
    is_x = (lane // q4) % 2 == 0

    def head_norm(u, g):
        sq = u * u
        hi = sq.astype(BF16)
        lo = (sq - hi.astype(F32)).astype(BF16)
        ms = jnp.dot(hi, average, preferred_element_type=F32) + jnp.dot(lo, average, preferred_element_type=F32)
        return u * lax.rsqrt(ms + token_eps) * g

    def turn(t):
        other = jnp.where(is_x, pltpu.roll(t, 128 - q4, 1), pltpu.roll(t, q4, 1))
        return t * cosb[...] + other * sinb[...]

    heads = width // 128
    last = Z // 2

    def ring(step, direction, which):
        buf = (kbuf, vbuf, cbuf)[which]
        side = 0 if direction == 1 else 1
        if direction == 1:
            src, dst = step, step + 1
        elif isinstance(step, int):
            src = 0 if step == 0 else last + step
            dst = last if step == last - 1 else last + step + 1
        else:
            src, dst = last + step, last + step + 1
        return copy_to(
            buf.at[src], buf.at[dst], r_send.at[side, which, step], r_recv.at[side, which, step], sp=zz(direction)
        )

    vbuf[0] = (accs[0] + product(block, wv, yy(2))).astype(BF16)
    for direction in (1, -1):
        ring(0, direction, 1).start()
    gk = jnp.concatenate([kg[...]] * (width // hw), axis=1)
    u = head_norm(accs[1] + product(block, wk, yy(2)), gk)
    for h in range(heads):
        kbuf[0, :, h * 128 : (h + 1) * 128] = turn(u[:, h * 128 : (h + 1) * 128]).astype(BF16)
    for direction in (1, -1):
        ring(0, direction, 0).start()

    for c in stage2n:
        c.wait_recv()
    fulln[y] = farn[0] + farn[1]
    stage3n = third_stage(fulln, 1)
    for c in stage3n:
        c.start()

    gq = jnp.concatenate([qg[...]] * (width // hw), axis=1)
    u = head_norm(accs[2] + product(block, wq, yy(2)), gq)
    for h in range(heads):
        t = turn(u[:, h * 128 : (h + 1) * 128]) * (hw ** -0.5)
        qz[h, pl.ds(0, LR), :] = jnp.where(lane < hw, t, 0.0).astype(BF16)
        qz[h, pl.ds(LR, LR), :] = jnp.where(lane < hw, 0.0, t).astype(BF16)

    for c in stage3n:
        c.wait_recv()
    own = jnp.concatenate(
        [
            (
                xc[:, b * cb : (b + 1) * cb] * (gain[:, b * cb : (b + 1) * cb] * (1.0 + row_of(fulln, b, 2)))
                + row_of(fulln, b, 1)
            ).astype(BF16)
            for b in range(Y)
        ],
        axis=1,
    )
    u = head_norm(jnp.dot(own, wk[...], preferred_element_type=F32), gk)
    cbuf[0, :, 0:width] = u.astype(BF16)
    cbuf[0, :, width : 2 * width] = jnp.dot(own, wv[...], preferred_element_type=F32).astype(BF16)
    for direction in (1, -1):
        ring(0, direction, 2).start()

    wh = wo.shape[1] // 2
    loads[17].wait()
    wo_sends = y_copies(wo.at[y], wo, w_send, w_recv, pl.ds(0, wh), pl.ds(wh, wh))
    for c in wo_sends:
        c.start()

    numer[...] = jnp.zeros_like(numer)
    tot[...] = jnp.zeros_like(tot)

    def attend(h, keys, values, extra):
        s = lax.dot_general(qz[h], keys, (((1,), (1,)), ((), ())), preferred_element_type=F32)
        if extra is not None:
            s = s + extra
        w = jnp.exp(s)
        t = w[:, 0:128]
        for j in range(1, w.shape[1] // 128):
            t = t + w[:, j * 128 : (j + 1) * 128]
        tot[h] = tot[h] + t
        numer[h] = numer[h] + jnp.dot(w.astype(BF16), values, preferred_element_type=F32)

    def attend_head(slot, h):
        hc = slice(h * 128, (h + 1) * 128)
        attend(h, kbuf[slot, :, hc], vbuf[slot, :, hc], None)

    def attend_context(low, high):
        for h in range(heads):
            keys = cbuf[low:high, :, h * 128 : (h + 1) * 128].reshape((high - low) * CR, 128)
            values = cbuf[low:high, :, width + h * 128 : width + (h + 1) * 128].reshape((high - low) * CR, 128)
            attend(h, keys, values, lift[:, h : h + 1])

    def receive(s, direction, which, forward=True):
        ring(s - 1, direction, which).wait_recv()
        if forward:
            ring(s, direction, which).start()

    def pass_on(s, units):
        for n, (which, direction) in enumerate(((1, 1), (1, -1), (0, 1), (0, -1))):
            receive(s, direction, which)
            if n < len(units):
                attend_head(*units[n])
        for direction in (1, -1):
            receive(s, direction, 2)

    def earlier(s):
        return [(slot, h) for slot in (s - 1, last + s - 1) for h in range(heads)]

    def hop(s, carry):
        pass_on(s, earlier(s))
        return carry

    mid = last // 2
    pass_on(1, [(0, h) for h in range(heads)])
    lax.fori_loop(2, mid, hop, 0)
    wo_sends[0].wait_recv()
    wo_sends[1].wait_recv()
    wo_forward = y_forward(wo, w_send, w_recv, pl.ds(0, wh), pl.ds(wh, wh))
    for c in wo_forward:
        c.start()
    lax.fori_loop(mid, last - 1, hop, 0)
    s = last - 1
    units = earlier(s)
    receive(s, -1, 1)
    attend_head(*units[0])
    receive(s, 1, 0)
    receive(s, 1, 2)
    attend_head(*units[1])
    receive(s, 1, 1, False)
    receive(s, -1, 0, False)
    receive(s, -1, 2, False)
    for slot, h in units[2:] + earlier(s + 1):
        attend_head(slot, h)
    attend_context(0, last)
    ring(s, -1, 1).wait_recv()
    ring(s, 1, 0).wait_recv()
    for h in range(heads):
        attend_head(last, h)
    ring(s, 1, 2).wait_recv()
    attend_context(last, Z)

    for h in range(heads):
        total = jnp.sum(tot[h], axis=-1, keepdims=True)
        ratio = numer[h] / total
        mixed = ratio[0:LR] - lam[:, h : h + 1] * ratio[LR : 2 * LR]
        ms = jnp.mean(mixed * mixed, axis=-1, keepdims=True)
        res = (mixed * lax.rsqrt(ms + head_eps) * vg[...] * head_factor).astype(BF16)
        for k in range(Y):
            hosend[k, :, h * 128 : (h + 1) * 128] = res[k * rows : (k + 1) * rows]
    o_copies = []
    for n, d in enumerate((2, 1, 3)):
        c = copy_to(hosend.at[yy(d)], ho.at[y], o_send.at[n], o_recv.at[n], tp=yy(d))
        c.start()
        o_copies.append(c)
    for c in wo_sends[2:] + wo_forward:
        c.wait_recv()
    oacc[...] = jnp.dot(hosend[y], wo[y], preferred_element_type=F32)
    for m, d in ((2, -3), (1, -1)):
        o_copies[m].wait_recv()
        oacc[...] = oacc[...] + jnp.dot(ho[yy(d)], wo[yy(d)], preferred_element_type=F32)
    o_copies[0].wait_recv()
    for b in range(Y):
        cols = pl.ds(b * cb, cb)
        acc = oacc[:, cols] + jnp.dot(ho[yy(2)], wo[yy(2), :, cols], preferred_element_type=F32)
        out[:, cols] = (latent[:, cols].astype(F32) + row_of(fulln, b, 0) * acc).astype(BF16)

    sent = stage1 + stage1n + stage2 + stage2n + stage3 + stage3n + lat_sends + lat_forward + wo_sends + wo_forward
    for c in sent + o_copies:
        c.wait_send()
    for s in range(last - 1):
        for direction in (1, -1):
            for which in (0, 1, 2):
                ring(s, direction, which).wait_send()
    ring(last - 1, 1, 0).wait_send()
    ring(last - 1, 1, 2).wait_send()
    ring(last - 1, -1, 1).wait_send()


def on_device(
    sizes, latent, context, cond, context_cond, norm_gain, mod_shift, mod_scale, mod_gate, w_query, w_key, w_value,
    query_gain, key_gain, mix_lambda, context_lift, value_gain, w_out,
):
    Z, Y = sizes
    rows, D = latent.shape
    cr = context.shape[0]
    LR = Y * rows
    width = w_query.shape[1]
    heads = width // 128
    rope = jnp.asarray(rope_table(query_gain.shape[0]))
    hbm = pl.BlockSpec(memory_space=pltpu.HBM)
    dma = pltpu.SemaphoreType.DMA
    V = pltpu.VMEM
    hb = lambda a: pltpu.with_memory_space_constraint(a, pltpu.HBM)
    operands = tuple(hb(a) for a in (
        latent, context, cond.reshape(1, -1), context_cond.reshape(1, -1), norm_gain.reshape(1, -1),
        mod_shift, mod_scale, mod_gate, query_gain.reshape(1, -1), key_gain.reshape(1, -1), value_gain.reshape(1, -1),
        mix_lambda.reshape(1, -1), context_lift.reshape(1, -1), rope, w_key, w_value, w_query, w_out,)
    )
    crit = 2 * mod_shift.shape[1] // 128
    rest = 2 * crit
    return pl.pallas_call(
        functools.partial(kernel, sizes),
        out_shape=jax.ShapeDtypeStruct((rows, D), BF16),
        in_specs=[hbm] * len(operands),
        out_specs=pl.BlockSpec(memory_space=pltpu.VMEM),
        scratch_shapes=[V(a.shape, a.dtype) for a in operands[:-1]]
        + [
            V((Y, w_out.shape[0], D), BF16),
            V((Y, rows, D), BF16), V((Y, rows, D), F32), V((cr, D), F32), V((3, LR, width), F32), V((rows, D), F32),
            V((8, crit, 128), F32), V((crit, 128), F32), V((2, crit, 128), F32), V((Y, crit, 128), F32),
            V((8, rest, 128), F32), V((rest, 128), F32), V((2, rest, 128), F32), V((Y, rest, 128), F32),
            V((LR, 128), F32), V((LR, 128), F32),
            V((heads, 2 * LR, 128), BF16), V((Z, LR, width), BF16), V((Z, LR, width), BF16), V((Z, cr, 2 * width), BF16),
            V((heads, 2 * LR, 128), F32), V((heads, 2 * LR, 128), F32),
            V((Y, rows, width), BF16), V((Y, rows, width), BF16),
            dma((len(operands),)), dma((2, 7)), dma((2, 7)), dma((2, 2)), dma((2, 2)), dma((2, 3)), dma((2, 3)),
            dma((6,)), dma((6,)), dma((6,)), dma((6,)), dma((2, 3, Z // 2)), dma((2, 3, Z // 2)), dma((3,)), dma((3,)),
        ],
        compiler_params=pltpu.CompilerParams(
            collective_id=0, has_side_effects=True, vmem_limit_bytes=48 * 1024 * 1024
        ),
    )(*operands)


def solution(mesh):
    placed = (
        P(("dp", "sp", "tp"), None),
        P(("dp", "sp"), None),
        P(("dp", "sp")),
        P("sp"),
        P(),
        P("sp", "tp"),
        P("sp", "tp"),
        P("sp", "tp"),
        P(None, "tp"),
        P(None, "tp"),
        P(None, "tp"),
        P(),
        P(),
        P("tp"),
        P("tp"),
        P(),
        P("tp", None),
    )
    sizes = (mesh.shape["sp"], mesh.shape["tp"])
    return jax.shard_map(
        functools.partial(on_device, sizes),
        mesh=mesh,
        in_specs=placed,
        out_specs=P(("dp", "sp", "tp"), None),
        check_vma=False,
    )
```

```python
import functools

import jax
import jax.numpy as jnp
import numpy as np
from jax import lax
from jax.experimental import pallas as pl
from jax.experimental.pallas import tpu as pltpu
from jax.sharding import PartitionSpec as P

GRID = 64
token_eps = 0.01
head_eps = 0.001
rope_base = 10000.0
head_factor = 0.8
MESH = pl.DeviceIdType.MESH
F32 = jnp.float32
BF16 = jnp.bfloat16


def rope_table(head_width):
    quarter = head_width // 4
    inverse = np.float32(rope_base) ** (-np.arange(quarter, dtype=np.float32) / np.float32(quarter))
    angles = (np.arange(GRID, dtype=np.float32)[:, None] * inverse).astype(np.float64)
    cos, sin = np.cos(angles), np.sin(angles)
    zero = np.zeros_like(cos)
    cos_row = np.concatenate([cos, cos, zero, zero], 1)
    cos_col = np.concatenate([zero, zero, cos, cos], 1)
    sin_row = np.concatenate([-sin, sin, zero, zero], 1)
    sin_col = np.concatenate([zero, zero, -sin, sin], 1)
    table = np.stack([np.stack([cos_row, cos_col]), np.stack([sin_row, sin_col])])
    return np.tile(table, (1, 1, 1, 2)).astype(np.float32)


def silu(v):
    return v / (1.0 + jnp.exp(-v))


def kernel(
    dims,
    latent_h, context_h, cond_h, cctx_h, gain_h, msh_h, msc_h, mga_h, qg_h, kg_h, vg_h, lam_h, lift_h, rope_h,
    wk_h, wv_h, wq_h, wo_h,
    out,
    latent, cond, cctx, gain, msh, msc, mga, qg, kg, vg, lam, lift, rope, wk, wv, wq,
    wo, lat, xi, accs, oacc, part, sums, far, full, partn, sumsn, farn, fulln, cosb, sinb, qz, kbuf, vbuf, ctxg, cinv, caccs, kctx, vctx,
    numer, tot, hosend, ho,
    lsem, p_send, p_recv, f_send, f_recv, c_send, c_recv, y_send, y_recv, w_send, w_recv, r_send, r_recv, o_send, o_recv,
    x_send, x_recv, g_send, g_recv,
):
    Z, Y = dims
    z, y = lax.axis_index("sp"), lax.axis_index("tp")

    def zz(d):
        return lax.rem(z + (d + Z), Z)

    def yy(d):
        return lax.rem(y + (d + Y), Y)

    T = msh.shape[1] // 128
    cb = T * 128

    def columns(b):
        return pl.ds(pl.multiple_of(b * cb, cb), cb)

    barrier = pltpu.get_barrier_semaphore()
    z_peers = [4, -4, 3, -3, 2, -2, 1, -1]
    for d in z_peers:
        pl.semaphore_signal(barrier, inc=1, device_id={"sp": zz(d)}, device_id_type=MESH)
    for d in (2, 1, 3):
        pl.semaphore_signal(barrier, inc=1, device_id={"tp": yy(d)}, device_id_type=MESH)

    pairs = [
        (cond_h, cond), (cctx_h, cctx), (msh_h, msh), (msc_h, msc), (mga_h, mga), (latent_h, latent),
        (context_h.at[:, columns(y)], ctxg.at[y, 0]), (rope_h, rope), (gain_h, gain), (qg_h, qg), (kg_h, kg), (vg_h, vg), (lam_h, lam), (lift_h, lift),
        (wv_h, wv), (wk_h, wk), (wq_h, wq), (wo_h, wo.at[y]),
    ]
    loads = [pltpu.make_async_copy(src, dst, lsem.at[n]) for n, (src, dst) in enumerate(pairs)]
    for copy in loads:
        copy.start()
    for copy in loads[:5]:
        copy.wait()

    rows16 = lax.broadcasted_iota(jnp.int32, (16, 128), 0)
    a0 = silu(cond[...].astype(F32))
    a1 = silu(cctx[...].astype(F32))
    acts = jnp.where(rows16 == 0, a0, jnp.where(rows16 == 1, a1, 0.0)).astype(BF16)
    p_sh = jnp.dot(acts, msh[...], preferred_element_type=F32)
    p_sc = jnp.dot(acts, msc[...], preferred_element_type=F32)
    p_ga = jnp.dot(acts, mga[...], preferred_element_type=F32)
    for j in range(T):
        js = slice(j * 128, (j + 1) * 128)
        part[0, j : j + 1, :] = p_sh[0:1, js]
        part[0, T + j : T + j + 1, :] = p_sc[0:1, js]
        partn[0, j : j + 1, :] = p_ga[0:1, js]
        partn[0, T + j : T + j + 1, :] = p_sh[1:2, js]
        partn[0, 2 * T + j : 2 * T + j + 1, :] = p_sc[1:2, js]
        partn[0, 3 * T + j : 3 * T + j + 1, :] = jnp.zeros((1, 128), F32)
    loads[5].wait()

    pl.semaphore_wait(barrier, len(z_peers) + 3)

    def copy_to(src, dst, ssem, rsem, **where):
        return pltpu.make_async_remote_copy(
            src_ref=src, dst_ref=dst, send_sem=ssem, recv_sem=rsem, device_id=where, device_id_type=MESH
        )

    offs = [-4, 3, -3, 2, -2, 1, -1]

    def first_stage(buf, g):
        return [
            copy_to(buf.at[0], buf.at[n + 1], p_send.at[g, n], p_recv.at[g, n], sp=zz(-d)) for n, d in enumerate(offs)
        ]

    stage1 = first_stage(part, 0)
    stage1n = first_stage(partn, 1)
    for c in stage1:
        c.start()

    rows = latent.shape[0]
    half = rows // 2
    top, bottom = pl.ds(0, half), pl.ds(half, half)

    def y_copies(src, slots, send, recv, first, second):
        return [
            copy_to(src.at[first], slots.at[y, first], send.at[0], recv.at[0], tp=yy(1)),
            copy_to(src.at[second], slots.at[y, second], send.at[1], recv.at[1], tp=yy(-1)),
            copy_to(src.at[second], slots.at[y, second], send.at[2], recv.at[2], tp=yy(1)),
            copy_to(src.at[first], slots.at[y, first], send.at[3], recv.at[3], tp=yy(-1)),
        ]

    def y_forward(slots, send, recv, first, second):
        return [
            copy_to(slots.at[yy(-1), first], slots.at[yy(-1), first], send.at[4], recv.at[4], tp=yy(1)),
            copy_to(slots.at[yy(1), second], slots.at[yy(1), second], send.at[5], recv.at[5], tp=yy(-1)),
        ]

    lat_sends = y_copies(latent, lat, y_send, y_recv, top, bottom)
    for c in lat_sends:
        c.start()
    for c in stage1n:
        c.start()

    def unit(x):
        xf = x.astype(F32)
        return xf * lax.rsqrt(jnp.mean(xf * xf, axis=-1, keepdims=True) + token_eps)

    width = wq.shape[1]
    hw = qg.shape[1]
    LR = Y * rows
    CR = ctxg.shape[2]
    xi[y] = unit(latent[...])

    def window(buf):
        t = buf[0]
        for n in range(len(offs)):
            t = t + buf[n + 1]
        return t

    def second_stage(src, dst, g):
        return [
            copy_to(src, dst.at[n], f_send.at[g, n], f_recv.at[g, n], sp=zz(d)) for n, d in enumerate((4, -4))
        ]

    for c in stage1:
        c.wait_recv()
    sums[...] = window(part)
    stage2 = second_stage(sums, far, 0)
    for c in stage2:
        c.start()
    for c in stage1n:
        c.wait_recv()
    sumsn[...] = window(partn)
    stage2n = second_stage(sumsn, farn, 1)
    for c in stage2n:
        c.start()

    reach = 4
    loads[6].wait()

    def context_copy(src, dst, to):
        return copy_to(ctxg.at[y, src], ctxg.at[y, dst], x_send.at[dst], x_recv.at[dst], sp=zz(to))

    near = {}
    for d in range(reach, 0, -1):
        for o in (d, Z - d):
            near[o] = context_copy(0, o, -o if o <= reach else Z - o)
            near[o].start()

    lat_sends[0].wait_recv()
    lat_sends[1].wait_recv()
    lat_forward = y_forward(lat, y_send, y_recv, top, bottom)
    for c in lat_forward:
        c.start()

    gi = lax.broadcasted_iota(jnp.int32, (width, width), 0) // hw
    gj = lax.broadcasted_iota(jnp.int32, (width, width), 1) // hw
    average = jnp.where(gi == gj, 1.0 / hw, 0.0).astype(BF16)
    for copy in loads[7:14]:
        copy.wait()
    for k in range(Y):
        at = pl.ds(k * rows, rows)
        cosb[at, :] = rope[0, 0, pl.ds(Y * z + k, 1), :] + rope[0, 1]
        sinb[at, :] = rope[1, 0, pl.ds(Y * z + k, 1), :] + rope[1, 1]
    lat_sends[2].wait_recv()
    lat_sends[3].wait_recv()
    for d in (1, -1):
        xi[yy(d)] = unit(lat[yy(d)])

    def third_stage(buf, g):
        return [
            copy_to(buf.at[y], buf.at[y], c_send.at[g, n], c_recv.at[g, n], tp=yy(d)) for n, d in enumerate((2, 1, 3))
        ]

    for c in stage2:
        c.wait_recv()
    full[y] = far[0] + far[1]
    stage3 = third_stage(full, 0)
    for c in stage3:
        c.start()
    near[reach].wait_recv()
    near[Z - reach].wait_recv()
    relayed = [context_copy(reach, reach + d, -d) for d in range(1, reach + 1)]
    relayed += [context_copy(Z - reach, Z - reach - d, d) for d in range(1, reach)]
    for c in relayed:
        c.start()
    for c in lat_forward:
        c.wait_recv()
    xi[yy(2)] = unit(lat[yy(2)])
    for copy in loads[14:17]:
        copy.wait()

    def row_of(buf, b, r):
        return jnp.concatenate([buf[b, r * T + j : r * T + j + 1, :] for j in range(T)], axis=1)

    def modulated(b):
        at = columns(b)
        scaled = gain[:, at] * (1.0 + row_of(full, b, 1))
        return (xi[:, :, at].reshape(LR, cb) * scaled + row_of(full, b, 0)).astype(BF16)

    def product(part_rows, weight, b):
        return jnp.dot(part_rows, weight[columns(b), :], preferred_element_type=F32)

    block = modulated(y)
    for n, weight in enumerate((wv, wk, wq)):
        accs[n] = product(block, weight, y)
    for m, d in ((2, -3), (1, -1)):
        stage3[m].wait_recv()
        block = modulated(yy(d))
        for n, weight in enumerate((wv, wk, wq)):
            accs[n] = accs[n] + product(block, weight, yy(d))
    stage3[0].wait_recv()
    block = modulated(yy(2))

    lane = lax.broadcasted_iota(jnp.int32, (1, 128), 1)
    q4 = hw // 4
    is_x = (lane // q4) % 2 == 0

    def head_norm(u, g):
        sq = u * u
        hi = sq.astype(BF16)
        lo = (sq - hi.astype(F32)).astype(BF16)
        ms = jnp.dot(hi, average, preferred_element_type=F32) + jnp.dot(lo, average, preferred_element_type=F32)
        return u * lax.rsqrt(ms + token_eps) * g

    def turn(t):
        other = jnp.where(is_x, pltpu.roll(t, 128 - q4, 1), pltpu.roll(t, q4, 1))
        return t * cosb[...] + other * sinb[...]

    heads = width // 128
    last = Z // 2

    def ring(step, direction, which):
        buf, h = (vbuf, kbuf)[which % 2], which // 2
        side = 0 if direction == 1 else 1
        if direction == 1:
            src, dst = step, step + 1
        elif isinstance(step, int):
            src = 0 if step == 0 else last + step
            dst = last if step == last - 1 else last + step + 1
        else:
            src, dst = last + step, last + step + 1
        return copy_to(
            buf.at[src, h], buf.at[dst, h], r_send.at[side, which, step], r_recv.at[side, which, step], sp=zz(direction)
        )

    gk = jnp.concatenate([kg[...]] * (width // hw), axis=1)
    v = accs[0] + product(block, wv, yy(2))
    for h in range(heads):
        vbuf[0, h] = v[:, h * 128 : (h + 1) * 128].astype(BF16)
    for direction in (1, -1):
        ring(0, direction, 0).start()
    u = head_norm(accs[1] + product(block, wk, yy(2)), gk)
    for h in range(heads):
        kbuf[0, h] = turn(u[:, h * 128 : (h + 1) * 128]).astype(BF16)
        for direction in (1, -1):
            if h > 0:
                ring(0, direction, 2 * h).start()
        for direction in (1, -1):
            ring(0, direction, 2 * h + 1).start()

    for c in stage2n:
        c.wait_recv()
    fulln[y] = farn[0] + farn[1]
    stage3n = third_stage(fulln, 1)
    for c in stage3n:
        c.start()

    gq = jnp.concatenate([qg[...]] * (width // hw), axis=1)
    u = head_norm(accs[2] + product(block, wq, yy(2)), gq)
    for h in range(heads):
        t = turn(u[:, h * 128 : (h + 1) * 128]) * (hw ** -0.5)
        qz[h, pl.ds(0, LR), :] = jnp.where(lane < hw, t, 0.0).astype(BF16)
        qz[h, pl.ds(LR, LR), :] = jnp.where(lane < hw, 0.0, t).astype(BF16)

    for n, c in near.items():
        if n not in (reach, Z - reach):
            c.wait_recv()
    for c in relayed:
        c.wait_recv()
    zh = Z // 2
    ctx_sends = y_copies(ctxg.at[y], ctxg, g_send, g_recv, pl.ds(0, zh), pl.ds(zh, zh))
    for c in ctx_sends:
        c.start()
    for c in stage3n:
        c.wait_recv()

    wh = wo.shape[1] // 2
    loads[17].wait()
    wo_sends = y_copies(wo.at[y], wo, w_send, w_recv, pl.ds(0, wh), pl.ds(wh, wh))
    for c in wo_sends:
        c.start()

    numer[...] = jnp.zeros_like(numer)
    tot[...] = jnp.zeros_like(tot)

    def attend(h, keys, values, extra):
        s = lax.dot_general(qz[h], keys, (((1,), (1,)), ((), ())), preferred_element_type=F32)
        if extra is not None:
            s = s + extra
        w = jnp.exp(s)
        t = w[:, 0:128]
        for j in range(1, w.shape[1] // 128):
            t = t + w[:, j * 128 : (j + 1) * 128]
        tot[h] = tot[h] + t
        numer[h] = numer[h] + jnp.dot(w.astype(BF16), values, preferred_element_type=F32)

    def attend_head(slot, h):
        attend(h, kbuf[slot, h], vbuf[slot, h], None)

    def receive(s, direction, which, forward=True):
        ring(s - 1, direction, which).wait_recv()
        if forward:
            ring(s, direction, which).start()

    def pass_on(s, units):
        per = -(-len(units) // (2 * heads))
        for which in range(2 * heads):
            for direction in (1, -1):
                receive(s, direction, which)
            for unit_of in units[which * per : (which + 1) * per]:
                unit_of()

    def earlier(s):
        return [functools.partial(attend_head, slot, h) for h in range(heads) for slot in (s - 1, last + s - 1)]

    def hop(s, carry):
        pass_on(s, earlier(s))
        return carry

    NC = Z * CR

    def context_scale():
        ms = jnp.zeros((NC, 1), F32)
        for b in range(Y):
            xf = ctxg[b].reshape(NC, cb).astype(F32)
            ms = ms + jnp.sum(xf * xf, axis=-1, keepdims=True)
        cinv[...] = jnp.broadcast_to(lax.rsqrt(ms / (Y * cb) + token_eps), (NC, 128))

    def context_block(b):
        at = slice(b * cb, (b + 1) * cb)
        wide = jnp.concatenate([cinv[...]] * T, axis=1)
        scaled = gain[:, at] * (1.0 + row_of(fulln, b, 2))
        rows_b = (ctxg[b].reshape(NC, cb).astype(F32) * wide * scaled + row_of(fulln, b, 1)).astype(BF16)
        for n, weight in enumerate((wv, wk)):
            p = jnp.dot(rows_b, weight[at, :], preferred_element_type=F32)
            caccs[n] = p if b == 0 else caccs[n] + p

    def context_done():
        kctx[...] = head_norm(caccs[1], gk).astype(BF16)
        vctx[...] = caccs[0].astype(BF16)

    def attend_context(h):
        hs = slice(h * 128, (h + 1) * 128)
        attend(h, kctx[:, hs], vctx[:, hs], lift[:, h : h + 1])

    pass_on(1, [functools.partial(attend_head, 0, h) for h in range(heads)])
    ctx_sends[0].wait_recv()
    ctx_sends[1].wait_recv()
    ctx_forward = y_forward(ctxg, g_send, g_recv, pl.ds(0, zh), pl.ds(zh, zh))
    for c in ctx_forward:
        c.start()
    mid = last // 2
    lax.fori_loop(2, mid, hop, 0)
    for c in ctx_sends[2:] + ctx_forward:
        c.wait_recv()
    extra = [context_scale] + [functools.partial(context_block, b) for b in range(Y)] + [context_done]
    extra += [functools.partial(attend_context, h) for h in range(heads)]
    pass_on(mid, [f for pair in zip(earlier(mid), extra[:4]) for f in pair])
    wo_sends[0].wait_recv()
    wo_sends[1].wait_recv()
    wo_forward = y_forward(wo, w_send, w_recv, pl.ds(0, wh), pl.ds(wh, wh))
    for c in wo_forward:
        c.start()
    pass_on(mid + 1, [f for pair in zip(earlier(mid + 1), extra[4:]) for f in pair])
    lax.fori_loop(mid + 2, last - 1, hop, 0)
    s = last - 1
    units = earlier(s)
    for n in range(2 * heads):
        receive(s, 1 if n % 2 else -1, n)
        units[n]()
    for n in range(2 * heads):
        receive(s, -1 if n % 2 else 1, n, False)
    for f in earlier(s + 1):
        f()

    o_copies = []
    for h in range(heads):
        ring(s, -1, 2 * h).wait_recv()
        ring(s, 1, 2 * h + 1).wait_recv()
        attend_head(last, h)
        total = jnp.sum(tot[h], axis=-1, keepdims=True)
        ratio = numer[h] / total
        mixed = ratio[0:LR] - lam[:, h : h + 1] * ratio[LR : 2 * LR]
        ms = jnp.mean(mixed * mixed, axis=-1, keepdims=True)
        res = (mixed * lax.rsqrt(ms + head_eps) * vg[...] * head_factor).astype(BF16)
        for k in range(Y):
            hosend[h, k] = res[k * rows : (k + 1) * rows]
        for n, d in enumerate((2, 1, 3)):
            c = copy_to(hosend.at[h, yy(d)], ho.at[h, y], o_send.at[h, n], o_recv.at[h, n], tp=yy(d))
            c.start()
            o_copies.append(c)
    for c in wo_sends[2:] + wo_forward:
        c.wait_recv()

    def piece(buf, k):
        return jnp.concatenate([buf[h, k] for h in range(heads)], axis=1)

    oacc[...] = jnp.dot(piece(hosend, y), wo[y], preferred_element_type=F32)
    for m, d in ((2, -3), (1, -1)):
        for h in range(heads):
            o_copies[3 * h + m].wait_recv()
        oacc[...] = oacc[...] + jnp.dot(piece(ho, yy(d)), wo[yy(d)], preferred_element_type=F32)
    for h in range(heads):
        o_copies[3 * h].wait_recv()
    lasts = piece(ho, yy(2))
    for b in range(Y):
        cols = pl.ds(b * cb, cb)
        acc = oacc[:, cols] + jnp.dot(lasts, wo[yy(2), :, cols], preferred_element_type=F32)
        out[:, cols] = (latent[:, cols].astype(F32) + row_of(fulln, b, 0) * acc).astype(BF16)

    sent = stage1 + stage1n + stage2 + stage2n + stage3 + stage3n + lat_sends + lat_forward + wo_sends + wo_forward
    for c in sent + o_copies + list(near.values()) + relayed + ctx_sends + ctx_forward:
        c.wait_send()
    for step in range(last - 1):
        for direction in (1, -1):
            for which in range(2 * heads):
                ring(step, direction, which).wait_send()
    for h in range(heads):
        ring(last - 1, -1, 2 * h).wait_send()
        ring(last - 1, 1, 2 * h + 1).wait_send()


def on_device(
    sizes, latent, context, cond, context_cond, norm_gain, mod_shift, mod_scale, mod_gate, w_query, w_key, w_value,
    query_gain, key_gain, mix_lambda, context_lift, value_gain, w_out,
):
    Z, Y = sizes
    rows, D = latent.shape
    cr = context.shape[0]
    LR = Y * rows
    width = w_query.shape[1]
    heads = width // 128
    rope = jnp.asarray(rope_table(query_gain.shape[0]))
    hbm = pl.BlockSpec(memory_space=pltpu.HBM)
    dma = pltpu.SemaphoreType.DMA
    V = pltpu.VMEM
    hb = lambda a: pltpu.with_memory_space_constraint(a, pltpu.HBM)
    operands = tuple(hb(a) for a in (
        latent, context, cond.reshape(1, -1), context_cond.reshape(1, -1), norm_gain.reshape(1, -1),
        mod_shift, mod_scale, mod_gate, query_gain.reshape(1, -1), key_gain.reshape(1, -1), value_gain.reshape(1, -1),
        mix_lambda.reshape(1, -1), context_lift.reshape(1, -1), rope, w_key, w_value, w_query, w_out,)
    )
    crit = 2 * mod_shift.shape[1] // 128
    rest = 2 * crit
    return pl.pallas_call(
        functools.partial(kernel, sizes),
        out_shape=jax.ShapeDtypeStruct((rows, D), BF16),
        in_specs=[hbm] * len(operands),
        out_specs=pl.BlockSpec(memory_space=pltpu.VMEM),
        scratch_shapes=[V(a.shape, a.dtype) for n, a in enumerate(operands[:-1]) if n != 1]
        + [
            V((Y, w_out.shape[0], D), BF16),
            V((Y, rows, D), BF16), V((Y, rows, D), F32), V((3, LR, width), F32), V((rows, D), F32),
            V((8, crit, 128), F32), V((crit, 128), F32), V((2, crit, 128), F32), V((Y, crit, 128), F32),
            V((8, rest, 128), F32), V((rest, 128), F32), V((2, rest, 128), F32), V((Y, rest, 128), F32),
            V((LR, 128), F32), V((LR, 128), F32),
            V((heads, 2 * LR, 128), BF16), V((Z, heads, LR, 128), BF16), V((Z, heads, LR, 128), BF16),
            V((Y, Z, cr, D // Y), BF16), V((Z * cr, 128), F32), V((2, Z * cr, width), F32), V((Z * cr, width), BF16),
            V((Z * cr, width), BF16),
            V((heads, 2 * LR, 128), F32), V((heads, 2 * LR, 128), F32),
            V((heads, Y, rows, 128), BF16), V((heads, Y, rows, 128), BF16),
            dma((len(operands),)), dma((2, 7)), dma((2, 7)), dma((2, 2)), dma((2, 2)), dma((2, 3)), dma((2, 3)),
            dma((6,)), dma((6,)), dma((6,)), dma((6,)), dma((2, 2 * heads, Z // 2)), dma((2, 2 * heads, Z // 2)), dma((heads, 3)), dma((heads, 3)),
            dma((Z,)), dma((Z,)), dma((6,)), dma((6,)),
        ],
        compiler_params=pltpu.CompilerParams(
            collective_id=0, has_side_effects=True, vmem_limit_bytes=48 * 1024 * 1024
        ),
    )(*operands)


def solution(mesh):
    placed = (
        P(("dp", "sp", "tp"), None),
        P(("dp", "sp"), None),
        P(("dp", "sp")),
        P("sp"),
        P(),
        P("sp", "tp"),
        P("sp", "tp"),
        P("sp", "tp"),
        P(None, "tp"),
        P(None, "tp"),
        P(None, "tp"),
        P(),
        P(),
        P("tp"),
        P("tp"),
        P(),
        P("tp", None),
    )
    sizes = (mesh.shape["sp"], mesh.shape["tp"])
    return jax.shard_map(
        functools.partial(on_device, sizes),
        mesh=mesh,
        in_specs=placed,
        out_specs=P(("dp", "sp", "tp"), None),
        check_vma=False,
    )
```

```python
import functools

import jax
import jax.numpy as jnp
import numpy as np
from jax import lax
from jax.experimental import pallas as pl
from jax.experimental.pallas import tpu as pltpu
from jax.sharding import PartitionSpec as P

GRID = 64
token_eps = 0.01
head_eps = 0.001
rope_base = 10000.0
head_factor = 0.8
MESH = pl.DeviceIdType.MESH
F32 = jnp.float32
BF16 = jnp.bfloat16


def rope_table(head_width):
    quarter = head_width // 4
    inverse = np.float32(rope_base) ** (-np.arange(quarter, dtype=np.float32) / np.float32(quarter))
    angles = (np.arange(GRID, dtype=np.float32)[:, None] * inverse).astype(np.float64)
    cos, sin = np.cos(angles), np.sin(angles)
    zero = np.zeros_like(cos)
    cos_row = np.concatenate([cos, cos, zero, zero], 1)
    cos_col = np.concatenate([zero, zero, cos, cos], 1)
    sin_row = np.concatenate([-sin, sin, zero, zero], 1)
    sin_col = np.concatenate([zero, zero, -sin, sin], 1)
    table = np.stack([np.stack([cos_row, cos_col]), np.stack([sin_row, sin_col])])
    return np.tile(table, (1, 1, 1, 2)).astype(np.float32)


def silu(v):
    return v / (1.0 + jnp.exp(-v))


def kernel(
    dims,
    latent_h, context_h, cond_h, cctx_h, gain_h, msh_h, msc_h, mga_h, qg_h, kg_h, vg_h, lam_h, lift_h, rope_h,
    wk_h, wv_h, wq_h, wo_h,
    out,
    latent, context, cond, cctx, gain, msh, msc, mga, qg, kg, vg, lam, lift, rope, wk, wv, wq,
    wo, lat, xi, xc, accs, oacc, part, sums, far, full, partn, sumsn, farn, fulln, cosb, sinb, qz, kbuf, vbuf, cbuf,
    numer, tot, hosend, ho,
    lsem, p_send, p_recv, f_send, f_recv, c_send, c_recv, y_send, y_recv, w_send, w_recv, r_send, r_recv, o_send, o_recv, pace,
):
    Z, Y = dims
    z, y, dp = lax.axis_index("sp"), lax.axis_index("tp"), lax.axis_index("dp")
    partner = dp + 1 - 2 * lax.rem(dp, 2)

    def zz(d):
        return lax.rem(z + (d + Z), Z)

    def yy(d):
        return lax.rem(y + (d + Y), Y)

    barrier = pltpu.get_barrier_semaphore()
    z_peers = [4, -4, 3, -3, 2, -2, 1, -1]
    for d in z_peers:
        pl.semaphore_signal(barrier, inc=1, device_id={"sp": zz(d)}, device_id_type=MESH)
    for d in (2, 1, 3):
        pl.semaphore_signal(barrier, inc=1, device_id={"tp": yy(d)}, device_id_type=MESH)

    pl.semaphore_signal(barrier, inc=1, device_id={"dp": partner}, device_id_type=MESH)

    pairs = [
        (cond_h, cond), (cctx_h, cctx), (msh_h, msh), (msc_h, msc), (mga_h, mga), (latent_h, latent), (rope_h, rope),
        (gain_h, gain), (context_h, context), (qg_h, qg), (kg_h, kg), (vg_h, vg), (lam_h, lam), (lift_h, lift),
        (wv_h, wv), (wk_h, wk), (wq_h, wq), (wo_h, wo.at[y]),
    ]
    loads = [pltpu.make_async_copy(src, dst, lsem.at[n]) for n, (src, dst) in enumerate(pairs)]
    for copy in loads:
        copy.start()
    for copy in loads[:5]:
        copy.wait()

    rows16 = lax.broadcasted_iota(jnp.int32, (16, 128), 0)
    a0 = silu(cond[...].astype(F32))
    a1 = silu(cctx[...].astype(F32))
    acts = jnp.where(rows16 == 0, a0, jnp.where(rows16 == 1, a1, 0.0)).astype(BF16)
    p_sh = jnp.dot(acts, msh[...], preferred_element_type=F32)
    p_sc = jnp.dot(acts, msc[...], preferred_element_type=F32)
    p_ga = jnp.dot(acts, mga[...], preferred_element_type=F32)
    T = msh.shape[1] // 128
    for j in range(T):
        js = slice(j * 128, (j + 1) * 128)
        part[0, j : j + 1, :] = p_sh[0:1, js]
        part[0, T + j : T + j + 1, :] = p_sc[0:1, js]
        partn[0, j : j + 1, :] = p_ga[0:1, js]
        partn[0, T + j : T + j + 1, :] = p_sh[1:2, js]
        partn[0, 2 * T + j : 2 * T + j + 1, :] = p_sc[1:2, js]
        partn[0, 3 * T + j : 3 * T + j + 1, :] = jnp.zeros((1, 128), F32)
    loads[5].wait()

    pl.semaphore_wait(barrier, len(z_peers) + 4)

    def copy_to(src, dst, ssem, rsem, **where):
        return pltpu.make_async_remote_copy(
            src_ref=src, dst_ref=dst, send_sem=ssem, recv_sem=rsem, device_id=where, device_id_type=MESH
        )

    offs = [-4, 3, -3, 2, -2, 1, -1]

    def first_stage(buf, g):
        return [
            copy_to(buf.at[0], buf.at[n + 1], p_send.at[g, n], p_recv.at[g, n], sp=zz(-d)) for n, d in enumerate(offs)
        ]

    stage1 = first_stage(part, 0)
    stage1n = first_stage(partn, 1)
    for c in stage1:
        c.start()

    rows = latent.shape[0]
    half = rows // 2
    top, bottom = pl.ds(0, half), pl.ds(half, half)

    def y_copies(src, slots, send, recv, first, second):
        return [
            copy_to(src.at[first], slots.at[y, first], send.at[0], recv.at[0], tp=yy(1)),
            copy_to(src.at[second], slots.at[y, second], send.at[1], recv.at[1], tp=yy(-1)),
            copy_to(src.at[second], slots.at[y, second], send.at[2], recv.at[2], tp=yy(1)),
            copy_to(src.at[first], slots.at[y, first], send.at[3], recv.at[3], tp=yy(-1)),
        ]

    def y_forward(slots, send, recv, first, second):
        return [
            copy_to(slots.at[yy(-1), first], slots.at[yy(-1), first], send.at[4], recv.at[4], tp=yy(1)),
            copy_to(slots.at[yy(1), second], slots.at[yy(1), second], send.at[5], recv.at[5], tp=yy(-1)),
        ]

    lat_sends = y_copies(latent, lat, y_send, y_recv, top, bottom)
    for c in lat_sends:
        c.start()
    for c in stage1n:
        c.start()

    def unit(x):
        xf = x.astype(F32)
        return xf * lax.rsqrt(jnp.mean(xf * xf, axis=-1, keepdims=True) + token_eps)

    width = wq.shape[1]
    hw = qg.shape[1]
    LR = Y * rows
    CR = context.shape[0]
    xi[y] = unit(latent[...])

    def window(buf):
        t = buf[0]
        for n in range(len(offs)):
            t = t + buf[n + 1]
        return t

    def second_stage(src, dst, g):
        return [
            copy_to(src, dst.at[n], f_send.at[g, n], f_recv.at[g, n], sp=zz(d)) for n, d in enumerate((4, -4))
        ]

    for c in stage1:
        c.wait_recv()
    sums[...] = window(part)
    stage2 = second_stage(sums, far, 0)
    for c in stage2:
        c.start()
    for c in stage1n:
        c.wait_recv()
    sumsn[...] = window(partn)
    stage2n = second_stage(sumsn, farn, 1)
    for c in stage2n:
        c.start()

    lat_sends[0].wait_recv()
    lat_sends[1].wait_recv()
    lat_forward = y_forward(lat, y_send, y_recv, top, bottom)
    for c in lat_forward:
        c.start()

    gi = lax.broadcasted_iota(jnp.int32, (width, width), 0) // hw
    gj = lax.broadcasted_iota(jnp.int32, (width, width), 1) // hw
    average = jnp.where(gi == gj, 1.0 / hw, 0.0).astype(BF16)
    for copy in loads[6:14]:
        copy.wait()
    for k in range(Y):
        at = pl.ds(k * rows, rows)
        cosb[at, :] = rope[0, 0, pl.ds(Y * z + k, 1), :] + rope[0, 1]
        sinb[at, :] = rope[1, 0, pl.ds(Y * z + k, 1), :] + rope[1, 1]
    xc[...] = unit(context[...])
    lat_sends[2].wait_recv()
    lat_sends[3].wait_recv()
    for d in (1, -1):
        xi[yy(d)] = unit(lat[yy(d)])

    def third_stage(buf, g):
        return [
            copy_to(buf.at[y], buf.at[y], c_send.at[g, n], c_recv.at[g, n], tp=yy(d)) for n, d in enumerate((2, 1, 3))
        ]

    for c in stage2:
        c.wait_recv()
    full[y] = far[0] + far[1]
    stage3 = third_stage(full, 0)
    for c in stage3:
        c.start()
    for c in lat_forward:
        c.wait_recv()
    xi[yy(2)] = unit(lat[yy(2)])
    for copy in loads[14:17]:
        copy.wait()

    cb = T * 128

    def row_of(buf, b, r):
        return jnp.concatenate([buf[b, r * T + j : r * T + j + 1, :] for j in range(T)], axis=1)

    def columns(b):
        return pl.ds(pl.multiple_of(b * cb, cb), cb)

    def modulated(b):
        at = columns(b)
        scaled = gain[:, at] * (1.0 + row_of(full, b, 1))
        return (xi[:, :, at].reshape(LR, cb) * scaled + row_of(full, b, 0)).astype(BF16)

    def product(part_rows, weight, b):
        return jnp.dot(part_rows, weight[columns(b), :], preferred_element_type=F32)

    block = modulated(y)
    for n, weight in enumerate((wv, wk, wq)):
        accs[n] = product(block, weight, y)
    for c in stage2n:
        c.wait_recv()
    fulln[y] = farn[0] + farn[1]
    stage3n = third_stage(fulln, 1)
    for c in stage3n:
        c.start()

    for m, d in ((2, -3), (1, -1)):
        stage3[m].wait_recv()
        block = modulated(yy(d))
        for n, weight in enumerate((wv, wk, wq)):
            accs[n] = accs[n] + product(block, weight, yy(d))
    stage3[0].wait_recv()
    block = modulated(yy(2))

    lane = lax.broadcasted_iota(jnp.int32, (1, 128), 1)
    q4 = hw // 4
    is_x = (lane // q4) % 2 == 0

    def head_norm(u, g):
        sq = u * u
        hi = sq.astype(BF16)
        lo = (sq - hi.astype(F32)).astype(BF16)
        ms = jnp.dot(hi, average, preferred_element_type=F32) + jnp.dot(lo, average, preferred_element_type=F32)
        return u * lax.rsqrt(ms + token_eps) * g

    def turn(t):
        other = jnp.where(is_x, pltpu.roll(t, 128 - q4, 1), pltpu.roll(t, q4, 1))
        return t * cosb[...] + other * sinb[...]

    heads = width // 128
    last = Z // 2

    def ring(step, direction, which):
        buf = (kbuf, vbuf, cbuf)[which]
        side = 0 if direction == 1 else 1
        if direction == 1:
            src, dst = step, step + 1
        elif isinstance(step, int):
            src = 0 if step == 0 else last + step
            dst = last if step == last - 1 else last + step + 1
        else:
            src, dst = last + step, last + step + 1
        return copy_to(
            buf.at[src], buf.at[dst], r_send.at[side, which, step], r_recv.at[side, which, step], sp=zz(direction)
        )

    vbuf[0] = (accs[0] + product(block, wv, yy(2))).astype(BF16)
    for direction in (1, -1):
        ring(0, direction, 1).start()
    gk = jnp.concatenate([kg[...]] * (width // hw), axis=1)
    u = head_norm(accs[1] + product(block, wk, yy(2)), gk)
    for h in range(heads):
        kbuf[0, :, h * 128 : (h + 1) * 128] = turn(u[:, h * 128 : (h + 1) * 128]).astype(BF16)
    for direction in (1, -1):
        ring(0, direction, 0).start()

    gq = jnp.concatenate([qg[...]] * (width // hw), axis=1)
    u = head_norm(accs[2] + product(block, wq, yy(2)), gq)
    for h in range(heads):
        t = turn(u[:, h * 128 : (h + 1) * 128]) * (hw ** -0.5)
        first = jnp.where(lane < hw, t, 0.0).astype(BF16)
        second = jnp.where(lane < hw, 0.0, t).astype(BF16)
        for k in range(Y):
            qz[h, pl.ds(2 * k * rows, rows), :] = first[k * rows : (k + 1) * rows]
            qz[h, pl.ds((2 * k + 1) * rows, rows), :] = second[k * rows : (k + 1) * rows]

    for c in stage3n:
        c.wait_recv()
    own = jnp.concatenate(
        [
            (
                xc[:, b * cb : (b + 1) * cb] * (gain[:, b * cb : (b + 1) * cb] * (1.0 + row_of(fulln, b, 2)))
                + row_of(fulln, b, 1)
            ).astype(BF16)
            for b in range(Y)
        ],
        axis=1,
    )
    u = head_norm(jnp.dot(own, wk[...], preferred_element_type=F32), gk)
    cbuf[0, :, 0:width] = u.astype(BF16)
    cbuf[0, :, width : 2 * width] = jnp.dot(own, wv[...], preferred_element_type=F32).astype(BF16)
    for direction in (1, -1):
        ring(0, direction, 2).start()

    wh = wo.shape[1] // 2
    loads[17].wait()
    wo_sends = y_copies(wo.at[y], wo, w_send, w_recv, pl.ds(0, wh), pl.ds(wh, wh))
    for c in wo_sends:
        c.start()

    numer[...] = jnp.zeros_like(numer)
    tot[...] = jnp.zeros_like(tot)

    everyone = pl.ds(0, 2 * LR)

    def attend(h, keys, values, extra, at=everyone):
        s = lax.dot_general(qz[h, at, :], keys, (((1,), (1,)), ((), ())), preferred_element_type=F32)
        if extra is not None:
            s = s + extra
        w = jnp.exp(s)
        t = w[:, 0:128]
        for j in range(1, w.shape[1] // 128):
            t = t + w[:, j * 128 : (j + 1) * 128]
        tot[h, at, :] = tot[h, at, :] + t
        numer[h, at, :] = numer[h, at, :] + jnp.dot(w.astype(BF16), values, preferred_element_type=F32)

    def attend_head(slot, h, at=everyone):
        hc = slice(h * 128, (h + 1) * 128)
        attend(h, kbuf[slot, :, hc], vbuf[slot, :, hc], None, at)

    def attend_context(h, low, high, at=everyone):
        keys = cbuf[low:high, :, h * 128 : (h + 1) * 128].reshape((high - low) * CR, 128)
        values = cbuf[low:high, :, width + h * 128 : width + (h + 1) * 128].reshape((high - low) * CR, 128)
        attend(h, keys, values, lift[:, h : h + 1], at)

    def receive(s, direction, which, forward=True):
        ring(s - 1, direction, which).wait_recv()
        if forward:
            ring(s, direction, which).start()

    def in_step():
        pl.semaphore_signal(pace, inc=1, device_id={"dp": partner}, device_id_type=MESH)
        pl.semaphore_wait(pace, 1)

    def pass_on(s, units):
        in_step()
        for n, (which, direction) in enumerate(((1, 1), (1, -1), (0, 1), (0, -1))):
            receive(s, direction, which)
            if n < len(units):
                attend_head(*units[n])
        for direction in (1, -1):
            receive(s, direction, 2)

    def earlier(s):
        return [(slot, h) for slot in (s - 1, last + s - 1) for h in range(heads)]

    def hop(s, carry):
        pass_on(s, earlier(s))
        return carry

    mid = last // 2
    pass_on(1, [(0, h) for h in range(heads)])
    lax.fori_loop(2, mid, hop, 0)
    wo_sends[0].wait_recv()
    wo_sends[1].wait_recv()
    wo_forward = y_forward(wo, w_send, w_recv, pl.ds(0, wh), pl.ds(wh, wh))
    for c in wo_forward:
        c.start()
    lax.fori_loop(mid, last - 1, hop, 0)
    s = last - 1
    in_step()
    units = earlier(s)
    receive(s, -1, 1)
    attend_head(*units[0])
    receive(s, 1, 0)
    receive(s, 1, 2)
    attend_head(*units[1])
    receive(s, 1, 1, False)
    receive(s, -1, 0, False)
    receive(s, -1, 2, False)
    for slot, h in units[2:] + earlier(s + 1):
        attend_head(slot, h)
    for h in range(heads):
        attend_context(h, 0, last)
    ring(s, -1, 1).wait_recv()
    ring(s, 1, 0).wait_recv()
    o_copies = []
    for n, d in enumerate((2, 1, 3, 0)):
        k = yy(d)
        at = pl.ds(pl.multiple_of(2 * k * rows, 2 * rows), 2 * rows)
        for h in range(heads):
            attend_head(last, h, at)
        if n == 0:
            ring(s, 1, 2).wait_recv()
        for h in range(heads):
            attend_context(h, last, Z, at)
            ratio = numer[h, at, :] / jnp.sum(tot[h, at, :], axis=-1, keepdims=True)
            mixed = ratio[0:rows] - lam[:, h : h + 1] * ratio[rows : 2 * rows]
            ms = jnp.mean(mixed * mixed, axis=-1, keepdims=True)
            res = mixed * lax.rsqrt(ms + head_eps) * vg[...] * head_factor
            hosend[k, :, h * 128 : (h + 1) * 128] = res.astype(BF16)
        if d != 0:
            c = copy_to(hosend.at[k], ho.at[y], o_send.at[n], o_recv.at[n], tp=k)
            c.start()
            o_copies.append(c)
    for c in wo_sends[2:] + wo_forward:
        c.wait_recv()
    oacc[...] = jnp.dot(hosend[y], wo[y], preferred_element_type=F32)
    for m, d in ((2, -3), (1, -1)):
        o_copies[m].wait_recv()
        oacc[...] = oacc[...] + jnp.dot(ho[yy(d)], wo[yy(d)], preferred_element_type=F32)
    o_copies[0].wait_recv()
    for b in range(Y):
        cols = pl.ds(b * cb, cb)
        acc = oacc[:, cols] + jnp.dot(ho[yy(2)], wo[yy(2), :, cols], preferred_element_type=F32)
        out[:, cols] = (latent[:, cols].astype(F32) + row_of(fulln, b, 0) * acc).astype(BF16)

    sent = stage1 + stage1n + stage2 + stage2n + stage3 + stage3n + lat_sends + lat_forward + wo_sends + wo_forward
    for c in sent + o_copies:
        c.wait_send()
    for s in range(last - 1):
        for direction in (1, -1):
            for which in (0, 1, 2):
                ring(s, direction, which).wait_send()
    ring(last - 1, 1, 0).wait_send()
    ring(last - 1, 1, 2).wait_send()
    ring(last - 1, -1, 1).wait_send()


def on_device(
    sizes, latent, context, cond, context_cond, norm_gain, mod_shift, mod_scale, mod_gate, w_query, w_key, w_value,
    query_gain, key_gain, mix_lambda, context_lift, value_gain, w_out,
):
    Z, Y = sizes
    rows, D = latent.shape
    cr = context.shape[0]
    LR = Y * rows
    width = w_query.shape[1]
    heads = width // 128
    rope = jnp.asarray(rope_table(query_gain.shape[0]))
    hbm = pl.BlockSpec(memory_space=pltpu.HBM)
    dma = pltpu.SemaphoreType.DMA
    V = pltpu.VMEM
    hb = lambda a: pltpu.with_memory_space_constraint(a, pltpu.HBM)
    operands = tuple(hb(a) for a in (
        latent, context, cond.reshape(1, -1), context_cond.reshape(1, -1), norm_gain.reshape(1, -1),
        mod_shift, mod_scale, mod_gate, query_gain.reshape(1, -1), key_gain.reshape(1, -1), value_gain.reshape(1, -1),
        mix_lambda.reshape(1, -1), context_lift.reshape(1, -1), rope, w_key, w_value, w_query, w_out,)
    )
    crit = 2 * mod_shift.shape[1] // 128
    rest = 2 * crit
    return pl.pallas_call(
        functools.partial(kernel, sizes),
        out_shape=jax.ShapeDtypeStruct((rows, D), BF16),
        in_specs=[hbm] * len(operands),
        out_specs=pl.BlockSpec(memory_space=pltpu.VMEM),
        scratch_shapes=[V(a.shape, a.dtype) for a in operands[:-1]]
        + [
            V((Y, w_out.shape[0], D), BF16),
            V((Y, rows, D), BF16), V((Y, rows, D), F32), V((cr, D), F32), V((3, LR, width), F32), V((rows, D), F32),
            V((8, crit, 128), F32), V((crit, 128), F32), V((2, crit, 128), F32), V((Y, crit, 128), F32),
            V((8, rest, 128), F32), V((rest, 128), F32), V((2, rest, 128), F32), V((Y, rest, 128), F32),
            V((LR, 128), F32), V((LR, 128), F32),
            V((heads, 2 * LR, 128), BF16), V((Z, LR, width), BF16), V((Z, LR, width), BF16), V((Z, cr, 2 * width), BF16),
            V((heads, 2 * LR, 128), F32), V((heads, 2 * LR, 128), F32),
            V((Y, rows, width), BF16), V((Y, rows, width), BF16),
            dma((len(operands),)), dma((2, 7)), dma((2, 7)), dma((2, 2)), dma((2, 2)), dma((2, 3)), dma((2, 3)),
            dma((6,)), dma((6,)), dma((6,)), dma((6,)), dma((2, 3, Z // 2)), dma((2, 3, Z // 2)), dma((3,)), dma((3,)),
            pltpu.SemaphoreType.REGULAR,
        ],
        compiler_params=pltpu.CompilerParams(
            collective_id=0, has_side_effects=True, vmem_limit_bytes=48 * 1024 * 1024
        ),
    )(*operands)


def solution(mesh):
    placed = (
        P(("dp", "sp", "tp"), None),
        P(("dp", "sp"), None),
        P(("dp", "sp")),
        P("sp"),
        P(),
        P("sp", "tp"),
        P("sp", "tp"),
        P("sp", "tp"),
        P(None, "tp"),
        P(None, "tp"),
        P(None, "tp"),
        P(),
        P(),
        P("tp"),
        P("tp"),
        P(),
        P("tp", None),
    )
    sizes = (mesh.shape["sp"], mesh.shape["tp"])
    return jax.shard_map(
        functools.partial(on_device, sizes),
        mesh=mesh,
        in_specs=placed,
        out_specs=P(("dp", "sp", "tp"), None),
        check_vma=False,
    )
```

```python
import functools

import jax
import jax.numpy as jnp
import numpy as np
from jax import lax
from jax.experimental import pallas as pl
from jax.experimental.pallas import tpu as pltpu
from jax.sharding import PartitionSpec as P

GRID = 64
token_eps = 0.01
head_eps = 0.001
rope_base = 10000.0
head_factor = 0.8
MESH = pl.DeviceIdType.MESH
F32 = jnp.float32
BF16 = jnp.bfloat16


def rope_table(head_width):
    quarter = head_width // 4
    inverse = np.float32(rope_base) ** (-np.arange(quarter, dtype=np.float32) / np.float32(quarter))
    angles = (np.arange(GRID, dtype=np.float32)[:, None] * inverse).astype(np.float64)
    cos, sin = np.cos(angles), np.sin(angles)
    zero = np.zeros_like(cos)
    cos_row = np.concatenate([cos, cos, zero, zero], 1)
    cos_col = np.concatenate([zero, zero, cos, cos], 1)
    sin_row = np.concatenate([-sin, sin, zero, zero], 1)
    sin_col = np.concatenate([zero, zero, -sin, sin], 1)
    table = np.stack([np.stack([cos_row, cos_col]), np.stack([sin_row, sin_col])])
    return np.tile(table, (1, 1, 1, 2)).astype(np.float32)


def silu(v):
    return v / (1.0 + jnp.exp(-v))


def kernel(
    dims,
    latent_h, context_h, cond_h, cctx_h, gain_h, msh_h, msc_h, mga_h, qg_h, kg_h, vg_h, lam_h, lift_h, rope_h,
    wk_h, wv_h, wq_h, wo_h,
    out,
    latent, context, cond, cctx, gain, msh, msc, mga, qg, kg, vg, lam, lift, rope, wk, wv, wq,
    wo, lat, xi, xc, accs, oacc, part, sums, far, full, partn, sumsn, farn, fulln, cosb, sinb, qz, kbuf, vbuf, cbuf,
    numer, tot, hosend, ho,
    lsem, p_send, p_recv, f_send, f_recv, c_send, c_recv, y_send, y_recv, w_send, w_recv, r_send, r_recv, o_send, o_recv, pace,
):
    Z, Y = dims
    z, y, dp = lax.axis_index("sp"), lax.axis_index("tp"), lax.axis_index("dp")
    partner = dp + 1 - 2 * lax.rem(dp, 2)

    def zz(d):
        return lax.rem(z + (d + Z), Z)

    def yy(d):
        return lax.rem(y + (d + Y), Y)

    barrier = pltpu.get_barrier_semaphore()
    z_peers = [4, -4, 3, -3, 2, -2, 1, -1]
    for d in z_peers:
        pl.semaphore_signal(barrier, inc=1, device_id={"sp": zz(d)}, device_id_type=MESH)
    for d in (2, 1, 3):
        pl.semaphore_signal(barrier, inc=1, device_id={"tp": yy(d)}, device_id_type=MESH)

    pl.semaphore_signal(barrier, inc=1, device_id={"dp": partner}, device_id_type=MESH)

    pairs = [
        (cond_h, cond), (cctx_h, cctx), (msh_h, msh), (msc_h, msc), (mga_h, mga), (latent_h, latent), (rope_h, rope),
        (gain_h, gain), (context_h, context), (qg_h, qg), (kg_h, kg), (vg_h, vg), (lam_h, lam), (lift_h, lift),
        (wv_h, wv), (wk_h, wk), (wq_h, wq), (wo_h, wo.at[y]),
    ]
    loads = [pltpu.make_async_copy(src, dst, lsem.at[n]) for n, (src, dst) in enumerate(pairs)]
    for copy in loads:
        copy.start()
    for copy in loads[:5]:
        copy.wait()

    rows16 = lax.broadcasted_iota(jnp.int32, (16, 128), 0)
    a0 = silu(cond[...].astype(F32))
    a1 = silu(cctx[...].astype(F32))
    acts = jnp.where(rows16 == 0, a0, jnp.where(rows16 == 1, a1, 0.0)).astype(BF16)
    p_sh = jnp.dot(acts, msh[...], preferred_element_type=F32)
    p_sc = jnp.dot(acts, msc[...], preferred_element_type=F32)
    p_ga = jnp.dot(acts, mga[...], preferred_element_type=F32)
    T = msh.shape[1] // 128
    for j in range(T):
        js = slice(j * 128, (j + 1) * 128)
        part[0, j : j + 1, :] = p_sh[0:1, js]
        part[0, T + j : T + j + 1, :] = p_sc[0:1, js]
        partn[0, j : j + 1, :] = p_ga[0:1, js]
        partn[0, T + j : T + j + 1, :] = p_sh[1:2, js]
        partn[0, 2 * T + j : 2 * T + j + 1, :] = p_sc[1:2, js]
        partn[0, 3 * T + j : 3 * T + j + 1, :] = jnp.zeros((1, 128), F32)
    loads[5].wait()

    pl.semaphore_wait(barrier, len(z_peers) + 4)

    def copy_to(src, dst, ssem, rsem, **where):
        return pltpu.make_async_remote_copy(
            src_ref=src, dst_ref=dst, send_sem=ssem, recv_sem=rsem, device_id=where, device_id_type=MESH
        )

    offs = [-4, 3, -3, 2, -2, 1, -1]

    def first_stage(buf, g):
        return [
            copy_to(buf.at[0], buf.at[n + 1], p_send.at[g, n], p_recv.at[g, n], sp=zz(-d)) for n, d in enumerate(offs)
        ]

    stage1 = first_stage(part, 0)
    stage1n = first_stage(partn, 1)
    for c in stage1:
        c.start()

    rows = latent.shape[0]
    half = rows // 2
    top, bottom = pl.ds(0, half), pl.ds(half, half)

    def y_copies(src, slots, send, recv, first, second):
        return [
            copy_to(src.at[first], slots.at[y, first], send.at[0], recv.at[0], tp=yy(1)),
            copy_to(src.at[second], slots.at[y, second], send.at[1], recv.at[1], tp=yy(-1)),
            copy_to(src.at[second], slots.at[y, second], send.at[2], recv.at[2], tp=yy(1)),
            copy_to(src.at[first], slots.at[y, first], send.at[3], recv.at[3], tp=yy(-1)),
        ]

    def y_forward(slots, send, recv, first, second):
        return [
            copy_to(slots.at[yy(-1), first], slots.at[yy(-1), first], send.at[4], recv.at[4], tp=yy(1)),
            copy_to(slots.at[yy(1), second], slots.at[yy(1), second], send.at[5], recv.at[5], tp=yy(-1)),
        ]

    lat_sends = y_copies(latent, lat, y_send, y_recv, top, bottom)
    for c in lat_sends:
        c.start()
    for c in stage1n:
        c.start()

    def unit(x):
        xf = x.astype(F32)
        return xf * lax.rsqrt(jnp.mean(xf * xf, axis=-1, keepdims=True) + token_eps)

    width = wq.shape[1]
    hw = qg.shape[1]
    LR = Y * rows
    CR = context.shape[0]
    xi[y] = unit(latent[...])

    def window(buf):
        t = buf[0]
        for n in range(len(offs)):
            t = t + buf[n + 1]
        return t

    def second_stage(src, dst, g):
        return [
            copy_to(src, dst.at[n], f_send.at[g, n], f_recv.at[g, n], sp=zz(d)) for n, d in enumerate((4, -4))
        ]

    for c in stage1:
        c.wait_recv()
    sums[...] = window(part)
    stage2 = second_stage(sums, far, 0)
    for c in stage2:
        c.start()
    for c in stage1n:
        c.wait_recv()
    sumsn[...] = window(partn)
    stage2n = second_stage(sumsn, farn, 1)
    for c in stage2n:
        c.start()

    lat_sends[0].wait_recv()
    lat_sends[1].wait_recv()
    lat_forward = y_forward(lat, y_send, y_recv, top, bottom)
    for c in lat_forward:
        c.start()

    gi = lax.broadcasted_iota(jnp.int32, (width, width), 0) // hw
    gj = lax.broadcasted_iota(jnp.int32, (width, width), 1) // hw
    average = jnp.where(gi == gj, 1.0 / hw, 0.0).astype(BF16)
    for copy in loads[6:14]:
        copy.wait()
    for k in range(Y):
        at = pl.ds(k * rows, rows)
        cosb[at, :] = rope[0, 0, pl.ds(Y * z + k, 1), :] + rope[0, 1]
        sinb[at, :] = rope[1, 0, pl.ds(Y * z + k, 1), :] + rope[1, 1]
    xc[...] = unit(context[...])
    lat_sends[2].wait_recv()
    lat_sends[3].wait_recv()
    for d in (1, -1):
        xi[yy(d)] = unit(lat[yy(d)])

    def third_stage(buf, g):
        return [
            copy_to(buf.at[y], buf.at[y], c_send.at[g, n], c_recv.at[g, n], tp=yy(d)) for n, d in enumerate((2, 1, 3))
        ]

    for c in stage2:
        c.wait_recv()
    full[y] = far[0] + far[1]
    stage3 = third_stage(full, 0)
    for c in stage3:
        c.start()
    for c in lat_forward:
        c.wait_recv()
    xi[yy(2)] = unit(lat[yy(2)])
    for copy in loads[14:17]:
        copy.wait()

    cb = T * 128

    def row_of(buf, b, r):
        return jnp.concatenate([buf[b, r * T + j : r * T + j + 1, :] for j in range(T)], axis=1)

    def columns(b):
        return pl.ds(pl.multiple_of(b * cb, cb), cb)

    def modulated(b):
        at = columns(b)
        scaled = gain[:, at] * (1.0 + row_of(full, b, 1))
        return (xi[:, :, at].reshape(LR, cb) * scaled + row_of(full, b, 0)).astype(BF16)

    def product(part_rows, weight, b):
        return jnp.dot(part_rows, weight[columns(b), :], preferred_element_type=F32)

    block = modulated(y)
    for n, weight in enumerate((wv, wk, wq)):
        accs[n] = product(block, weight, y)
    for c in stage2n:
        c.wait_recv()
    fulln[y] = farn[0] + farn[1]
    stage3n = third_stage(fulln, 1)
    for c in stage3n:
        c.start()

    for m, d in ((2, -3), (1, -1)):
        stage3[m].wait_recv()
        block = modulated(yy(d))
        for n, weight in enumerate((wv, wk, wq)):
            accs[n] = accs[n] + product(block, weight, yy(d))
    stage3[0].wait_recv()
    block = modulated(yy(2))

    lane = lax.broadcasted_iota(jnp.int32, (1, 128), 1)
    q4 = hw // 4
    is_x = (lane // q4) % 2 == 0

    def head_norm(u, g):
        sq = u * u
        hi = sq.astype(BF16)
        lo = (sq - hi.astype(F32)).astype(BF16)
        ms = jnp.dot(hi, average, preferred_element_type=F32) + jnp.dot(lo, average, preferred_element_type=F32)
        return u * lax.rsqrt(ms + token_eps) * g

    def turn(t):
        other = jnp.where(is_x, pltpu.roll(t, 128 - q4, 1), pltpu.roll(t, q4, 1))
        return t * cosb[...] + other * sinb[...]

    heads = width // 128
    last = Z // 2

    def ring(step, direction, which):
        buf = (kbuf, vbuf, cbuf)[which]
        side = 0 if direction == 1 else 1
        if direction == 1:
            src, dst = step, step + 1
        elif isinstance(step, int):
            src = 0 if step == 0 else last + step
            dst = last if step == last - 1 else last + step + 1
        else:
            src, dst = last + step, last + step + 1
        return copy_to(
            buf.at[src], buf.at[dst], r_send.at[side, which, step], r_recv.at[side, which, step], sp=zz(direction)
        )

    vbuf[0] = (accs[0] + product(block, wv, yy(2))).astype(BF16)
    for direction in (1, -1):
        ring(0, direction, 1).start()
    gk = jnp.concatenate([kg[...]] * (width // hw), axis=1)
    u = head_norm(accs[1] + product(block, wk, yy(2)), gk)
    for h in range(heads):
        kbuf[0, :, h * 128 : (h + 1) * 128] = turn(u[:, h * 128 : (h + 1) * 128]).astype(BF16)
    for direction in (1, -1):
        ring(0, direction, 0).start()

    gq = jnp.concatenate([qg[...]] * (width // hw), axis=1)
    u = head_norm(accs[2] + product(block, wq, yy(2)), gq)
    for h in range(heads):
        t = turn(u[:, h * 128 : (h + 1) * 128]) * (hw ** -0.5)
        first = jnp.where(lane < hw, t, 0.0).astype(BF16)
        second = jnp.where(lane < hw, 0.0, t).astype(BF16)
        for k in range(Y):
            place = pl.multiple_of(lax.rem(k - y + (Y // 2 + Y), Y) * (2 * rows), 2 * rows)
            qz[h, pl.ds(place, rows), :] = first[k * rows : (k + 1) * rows]
            qz[h, pl.ds(place + rows, rows), :] = second[k * rows : (k + 1) * rows]

    for c in stage3n:
        c.wait_recv()
    own = jnp.concatenate(
        [
            (
                xc[:, b * cb : (b + 1) * cb] * (gain[:, b * cb : (b + 1) * cb] * (1.0 + row_of(fulln, b, 2)))
                + row_of(fulln, b, 1)
            ).astype(BF16)
            for b in range(Y)
        ],
        axis=1,
    )
    u = head_norm(jnp.dot(own, wk[...], preferred_element_type=F32), gk)
    cbuf[0, :, 0:width] = u.astype(BF16)
    cbuf[0, :, width : 2 * width] = jnp.dot(own, wv[...], preferred_element_type=F32).astype(BF16)
    for direction in (1, -1):
        ring(0, direction, 2).start()

    wh = wo.shape[1] // 2
    loads[17].wait()
    wo_sends = y_copies(wo.at[y], wo, w_send, w_recv, pl.ds(0, wh), pl.ds(wh, wh))
    for c in wo_sends:
        c.start()

    numer[...] = jnp.zeros_like(numer)
    tot[...] = jnp.zeros_like(tot)

    everyone = pl.ds(0, 2 * LR)

    def attend(h, keys, values, extra, at=everyone):
        s = lax.dot_general(qz[h, at, :], keys, (((1,), (1,)), ((), ())), preferred_element_type=F32)
        if extra is not None:
            s = s + extra
        w = jnp.exp(s)
        t = w[:, 0:128]
        for j in range(1, w.shape[1] // 128):
            t = t + w[:, j * 128 : (j + 1) * 128]
        tot[h, at, :] = tot[h, at, :] + t
        numer[h, at, :] = numer[h, at, :] + jnp.dot(w.astype(BF16), values, preferred_element_type=F32)

    def attend_head(slot, h, at=everyone):
        hc = slice(h * 128, (h + 1) * 128)
        attend(h, kbuf[slot, :, hc], vbuf[slot, :, hc], None, at)

    def attend_context(h, low, high, at=everyone):
        keys = cbuf[low:high, :, h * 128 : (h + 1) * 128].reshape((high - low) * CR, 128)
        values = cbuf[low:high, :, width + h * 128 : width + (h + 1) * 128].reshape((high - low) * CR, 128)
        attend(h, keys, values, lift[:, h : h + 1], at)

    def receive(s, direction, which, forward=True):
        ring(s - 1, direction, which).wait_recv()
        if forward:
            ring(s, direction, which).start()

    def in_step():
        pl.semaphore_signal(pace, inc=1, device_id={"dp": partner}, device_id_type=MESH)
        pl.semaphore_wait(pace, 1)

    def pass_on(s, units):
        in_step()
        for n, (which, direction) in enumerate(((1, 1), (1, -1), (0, 1), (0, -1))):
            receive(s, direction, which)
            if n < len(units):
                attend_head(*units[n])
        for direction in (1, -1):
            receive(s, direction, 2)

    def earlier(s):
        return [(slot, h) for slot in (s - 1, last + s - 1) for h in range(heads)]

    def hop(s, carry):
        pass_on(s, earlier(s))
        return carry

    mid = last // 2
    pass_on(1, [(0, h) for h in range(heads)])
    lax.fori_loop(2, mid, hop, 0)
    wo_sends[0].wait_recv()
    wo_sends[1].wait_recv()
    wo_forward = y_forward(wo, w_send, w_recv, pl.ds(0, wh), pl.ds(wh, wh))
    for c in wo_forward:
        c.start()
    lax.fori_loop(mid, last - 1, hop, 0)
    s = last - 1
    in_step()
    units = earlier(s)
    receive(s, -1, 1)
    attend_head(*units[0])
    receive(s, 1, 0)
    receive(s, 1, 2)
    attend_head(*units[1])
    receive(s, 1, 1, False)
    receive(s, -1, 0, False)
    receive(s, -1, 2, False)
    for slot, h in units[2:] + earlier(s + 1):
        attend_head(slot, h)
    for h in range(heads):
        attend_context(h, 0, last)
    ring(s, -1, 1).wait_recv()
    ring(s, 1, 0).wait_recv()
    o_copies = []
    for low, high in ((0, 1), (1, Y)):
        at = pl.ds(2 * low * rows, 2 * (high - low) * rows)
        for h in range(heads):
            attend_head(last, h, at)
        if low == 0:
            ring(s, 1, 2).wait_recv()
        for h in range(heads):
            attend_context(h, last, Z, at)
        for h in range(heads):
            for j in range(low, high):
                one, two = pl.ds(2 * j * rows, rows), pl.ds((2 * j + 1) * rows, rows)
                mixed = numer[h, one, :] / jnp.sum(tot[h, one, :], axis=-1, keepdims=True) - lam[:, h : h + 1] * (
                    numer[h, two, :] / jnp.sum(tot[h, two, :], axis=-1, keepdims=True)
                )
                ms = jnp.mean(mixed * mixed, axis=-1, keepdims=True)
                res = mixed * lax.rsqrt(ms + head_eps) * vg[...] * head_factor
                hosend[yy(j - Y // 2), :, h * 128 : (h + 1) * 128] = res.astype(BF16)
        for n, d in ((0, 2),) if low == 0 else ((1, 1), (2, 3)):
            c = copy_to(hosend.at[yy(d)], ho.at[y], o_send.at[n], o_recv.at[n], tp=yy(d))
            c.start()
            o_copies.append(c)
    for c in wo_sends[2:] + wo_forward:
        c.wait_recv()
    oacc[...] = jnp.dot(hosend[y], wo[y], preferred_element_type=F32)
    for m, d in ((2, -3), (1, -1)):
        o_copies[m].wait_recv()
        oacc[...] = oacc[...] + jnp.dot(ho[yy(d)], wo[yy(d)], preferred_element_type=F32)
    o_copies[0].wait_recv()
    for b in range(Y):
        cols = pl.ds(b * cb, cb)
        acc = oacc[:, cols] + jnp.dot(ho[yy(2)], wo[yy(2), :, cols], preferred_element_type=F32)
        out[:, cols] = (latent[:, cols].astype(F32) + row_of(fulln, b, 0) * acc).astype(BF16)

    sent = stage1 + stage1n + stage2 + stage2n + stage3 + stage3n + lat_sends + lat_forward + wo_sends + wo_forward
    for c in sent + o_copies:
        c.wait_send()
    for s in range(last - 1):
        for direction in (1, -1):
            for which in (0, 1, 2):
                ring(s, direction, which).wait_send()
    ring(last - 1, 1, 0).wait_send()
    ring(last - 1, 1, 2).wait_send()
    ring(last - 1, -1, 1).wait_send()


def on_device(
    sizes, latent, context, cond, context_cond, norm_gain, mod_shift, mod_scale, mod_gate, w_query, w_key, w_value,
    query_gain, key_gain, mix_lambda, context_lift, value_gain, w_out,
):
    Z, Y = sizes
    rows, D = latent.shape
    cr = context.shape[0]
    LR = Y * rows
    width = w_query.shape[1]
    heads = width // 128
    rope = jnp.asarray(rope_table(query_gain.shape[0]))
    hbm = pl.BlockSpec(memory_space=pltpu.HBM)
    dma = pltpu.SemaphoreType.DMA
    V = pltpu.VMEM
    hb = lambda a: pltpu.with_memory_space_constraint(a, pltpu.HBM)
    operands = tuple(hb(a) for a in (
        latent, context, cond.reshape(1, -1), context_cond.reshape(1, -1), norm_gain.reshape(1, -1),
        mod_shift, mod_scale, mod_gate, query_gain.reshape(1, -1), key_gain.reshape(1, -1), value_gain.reshape(1, -1),
        mix_lambda.reshape(1, -1), context_lift.reshape(1, -1), rope, w_key, w_value, w_query, w_out,)
    )
    crit = 2 * mod_shift.shape[1] // 128
    rest = 2 * crit
    return pl.pallas_call(
        functools.partial(kernel, sizes),
        out_shape=jax.ShapeDtypeStruct((rows, D), BF16),
        in_specs=[hbm] * len(operands),
        out_specs=pl.BlockSpec(memory_space=pltpu.VMEM),
        scratch_shapes=[V(a.shape, a.dtype) for a in operands[:-1]]
        + [
            V((Y, w_out.shape[0], D), BF16),
            V((Y, rows, D), BF16), V((Y, rows, D), F32), V((cr, D), F32), V((3, LR, width), F32), V((rows, D), F32),
            V((8, crit, 128), F32), V((crit, 128), F32), V((2, crit, 128), F32), V((Y, crit, 128), F32),
            V((8, rest, 128), F32), V((rest, 128), F32), V((2, rest, 128), F32), V((Y, rest, 128), F32),
            V((LR, 128), F32), V((LR, 128), F32),
            V((heads, 2 * LR, 128), BF16), V((Z, LR, width), BF16), V((Z, LR, width), BF16), V((Z, cr, 2 * width), BF16),
            V((heads, 2 * LR, 128), F32), V((heads, 2 * LR, 128), F32),
            V((Y, rows, width), BF16), V((Y, rows, width), BF16),
            dma((len(operands),)), dma((2, 7)), dma((2, 7)), dma((2, 2)), dma((2, 2)), dma((2, 3)), dma((2, 3)),
            dma((6,)), dma((6,)), dma((6,)), dma((6,)), dma((2, 3, Z // 2)), dma((2, 3, Z // 2)), dma((3,)), dma((3,)),
            pltpu.SemaphoreType.REGULAR,
        ],
        compiler_params=pltpu.CompilerParams(
            collective_id=0, has_side_effects=True, vmem_limit_bytes=48 * 1024 * 1024
        ),
    )(*operands)


def solution(mesh):
    placed = (
        P(("dp", "sp", "tp"), None),
        P(("dp", "sp"), None),
        P(("dp", "sp")),
        P("sp"),
        P(),
        P("sp", "tp"),
        P("sp", "tp"),
        P("sp", "tp"),
        P(None, "tp"),
        P(None, "tp"),
        P(None, "tp"),
        P(),
        P(),
        P("tp"),
        P("tp"),
        P(),
        P("tp", None),
    )
    sizes = (mesh.shape["sp"], mesh.shape["tp"])
    return jax.shard_map(
        functools.partial(on_device, sizes),
        mesh=mesh,
        in_specs=placed,
        out_specs=P(("dp", "sp", "tp"), None),
        check_vma=False,
    )
```
